512 devices in a mesh: kv: 64 (over z, y), tp: 8 (over x, core).
Axes of the slice: x: 4, y: 8, z: 8, core: 2. Of those that a mesh axis runs over, the one named last changes fastest.
Arguments:
- normed: bfloat16 [32768, 4096], P('kv'), may hold values from -16 to 16
- queries: bfloat16 [32768, 1024], P('kv', 'tp'), may hold values from -6 to 6
- keys: bfloat16 [32768, 64], P('kv'), may hold values from -6 to 6
- values: bfloat16 [32768, 64], P('kv'), may hold values from -6 to 6
- attended: bfloat16 [32768, 1024], P('kv', 'tp'), may hold values from -6 to 6
- cotangent: bfloat16 [32768, 1024], P('kv', 'tp'), may hold values from -24 to 24
- log_sum: float32 [32768, 16], P('kv', 'tp'), may hold values from 6 to 8
- chosen: int32 [512, 16], P('kv'), may hold values from -1 to 511, as said below
Outputs:
- grad_queries: bfloat16 [32768, 1024], P('kv', 'tp')
- grad_keys: float32 [32768, 64], P('kv')
- grad_values: float32 [32768, 64], P('kv')
- weight_grad: float32 [4096, 1024], P('kv', 'tp')
The draws below stay inside these ranges and needn't reach their ends.
Inputs may be any that keep to these rules, and one draw needn't show every extreme that they name: `chosen`: each row lists distinct key blocks, none after its own block, and always its own block; the listed entries come first and -1 fills the rest. A row lists from 8 to 16 blocks, fewer only where fewer blocks are open to it; on every index of kv some row lists 16 blocks where that many are open. The rows of one index of kv together list at most one block of each other index of kv's positions; every index of kv from 1 on lists a block of index 0 and a block of the index before it, and every index from half the axis on a block of the index half the axis before it.
All inputs are finite; a program needn't handle non-finite values.
Results may differ from the reference program's by a relative error of at most 0.007.
Values may be sent and summed in bfloat16 or wider, within the bound.
No kernel may reach another device: no remote copies, remote signals or barrier semaphores. Data moves between devices by JAX's collectives and lax.ppermute only.
A program may use at most 64 MiB of HBM per device.

```python
import jax
import jax.numpy as jnp
from jax import lax

D = 4096
HEADS = 16
HEAD_DIM = 64
BLOCK = 64
NSEL = 16
LEAST = 8
TOK_DEV = 512
TOKENS = 32768


def draw_chosen(key, part):
    device_count = TOKENS // TOK_DEV
    per_device = TOK_DEV // BLOCK
    block_count = TOKENS // BLOCK
    first_key = jax.random.fold_in(key, 11)
    second_key = jax.random.fold_in(key, 12)
    third_key = jax.random.fold_in(key, 13)
    fourth_key = jax.random.fold_in(key, 14)
    offsets = jax.random.randint(first_key, (device_count, device_count), 0, per_device)
    row_ids = jnp.arange(block_count, dtype=jnp.int32)
    col_ids = jnp.arange(block_count, dtype=jnp.int32)
    row_dev = row_ids // per_device
    col_dev = col_ids // per_device
    fetched = col_dev[None, :] * per_device + offsets[row_dev[:, None], col_dev[None, :]]
    local_open = (col_dev[None, :] == row_dev[:, None]) & (col_ids[None, :] <= row_ids[:, None])
    remote_open = (col_dev[None, :] < row_dev[:, None]) & (col_ids[None, :] == fetched)
    is_open = local_open | remote_open
    near = (col_dev[None, :] == row_dev[:, None] - 1) | (col_dev[None, :] == row_dev[:, None] - device_count // 2) | (col_dev[None, :] == 0)
    forced = (col_ids[None, :] == row_ids[:, None]) | remote_open & near
    noise = jax.random.randint(second_key, (block_count, block_count), 0, 4096)
    ranked = jnp.where(forced, 2 ** 28 + col_ids[None, :], jnp.where(is_open, noise * block_count + col_ids[None, :], -1 - col_ids[None, :]))
    top_values, picked = lax.top_k(ranked, NSEL)
    span_size = NSEL - LEAST + 1
    first_draw = jax.random.randint(third_key, (block_count,), 0, span_size)
    second_draw = jax.random.randint(fourth_key, (block_count,), 0, span_size)
    listed_count = LEAST + jnp.minimum(first_draw, second_draw)
    listed_count = jnp.where(row_ids % per_device == per_device - 1, NSEL, listed_count)
    slot_ids = jnp.arange(NSEL, dtype=jnp.int32)
    keep = (slot_ids[None, :] < listed_count[:, None]) & (top_values >= 0)
    return jnp.where(keep, picked, -1).astype(jnp.int32)


def strengthened(entries, stream_key, source, target, blocks, factor):
    def block_of(dim):
        return (jnp.arange(entries.shape[dim]) // (entries.shape[dim] // blocks)).reshape((-1,) + (1,) * (entries.ndim - 1 - dim))

    first = jax.random.permutation(stream_key, blocks)[block_of(target)]
    other_side = (block_of(target) + blocks // 2) % blocks
    return jnp.where((block_of(source) == first) | (block_of(source) == other_side), factor * entries, entries)


def block_levels(key, shape, pieces, smallest, largest):
    level = 1.0
    for position, blocks in pieces:
        heights = jax.random.uniform(jax.random.fold_in(jax.random.fold_in(key, 6), position), (blocks,), jnp.float32, smallest / len(pieces), largest / len(pieces))
        level = level * jnp.repeat(jnp.exp(heights), shape[position] // blocks).reshape((-1,) + (1,) * (len(shape) - 1 - position))
    return level


def scatter_about(stream_key, extent, scale, reach, shards=(), kind=jnp.bfloat16):
    entries = jax.random.normal(stream_key, extent, jnp.float32) * scale
    if len(shards) > 0:
        entries = block_levels(stream_key, extent, shards, -0.22, 0.18) * entries
    return jnp.clip(entries, min=-reach, max=reach).astype(kind)


def noise_with(stream_key, shape, deviation, reach, cuts, heavy, held_as=jnp.bfloat16):
    values = deviation * jax.random.normal(stream_key, shape, jnp.float32)
    if cuts:
        values = values * block_levels(stream_key, shape, cuts, -0.22, 0.18)
    return jnp.clip(strengthened(values, jax.random.fold_in(stream_key, 3), *heavy), -reach, reach).astype(held_as)


def setup_inputs(seed: int = 0) -> dict:
    key_list = jax.random.split(jax.random.key(seed), 9)
    normed = noise_with(key_list[0], (TOKENS, D), 1.0, 16.0, ((0, 64),), (0, 1, 64, 4.0))
    queries = scatter_about(key_list[1], (TOKENS, HEADS * HEAD_DIM), 1.0, 6.0, ((0, 64), (1, 8)))
    keys = scatter_about(key_list[2], (TOKENS, HEAD_DIM), 1.0, 6.0, ((0, 64),))
    values = scatter_about(key_list[3], (TOKENS, HEAD_DIM), 1.0, 6.0, ((0, 64),))
    attended = scatter_about(key_list[4], (TOKENS, HEADS * HEAD_DIM), 1.0, 6.0, ((0, 64), (1, 8)))
    cotangent = scatter_about(key_list[5], (TOKENS, HEADS * HEAD_DIM), 4.0, 24.0, ((0, 64), (1, 8)))
    log_sum = jnp.clip(6.0 + 2.0 * jax.random.uniform(key_list[6], (TOKENS, HEADS), jnp.float32) ** block_levels(key_list[6], (TOKENS, HEADS), ((0, 64), (1, 8)), -0.2, 0.2), 6.0, 8.0)
    chosen = draw_chosen(jax.random.fold_in(key_list[8], 71), 0)
    return {"normed": normed, "queries": queries, "keys": keys, "values": values, "attended": attended, "cotangent": cotangent, "log_sum": log_sum, "chosen": chosen}


def reference(normed, queries, keys, values, attended, cotangent, log_sum, chosen):
    block_count = TOKENS // BLOCK
    score_scale = HEAD_DIM ** -0.5
    query_matrix = queries.reshape(block_count, BLOCK, HEADS, HEAD_DIM)
    gradient_rows = cotangent.reshape(block_count, BLOCK, HEADS, HEAD_DIM)
    out_rows = attended.reshape(block_count, BLOCK, HEADS, HEAD_DIM)
    log_rows = log_sum.reshape(block_count, BLOCK, HEADS)
    pair_rows = jnp.concatenate([keys, values], axis=1).reshape(block_count, BLOCK, 2 * HEAD_DIM)
    offsets = jnp.arange(BLOCK, dtype=jnp.int32)

    def one_block(accumulated, block_id):
        listed_ids = chosen[block_id]
        listed = listed_ids >= 0
        safe_ids = jnp.where(listed, listed_ids, 0).astype(jnp.int32)
        picked = pair_rows[safe_ids].reshape(NSEL * BLOCK, 2 * HEAD_DIM).astype(jnp.float32)
        selected_keys = picked[:, :HEAD_DIM]
        selected_values = picked[:, HEAD_DIM:]
        query_block = query_matrix[block_id].astype(jnp.float32)
        grad_block = gradient_rows[block_id].astype(jnp.float32)
        out_block = out_rows[block_id].astype(jnp.float32)
        key_pos = (safe_ids[:, None] * BLOCK + offsets[None, :]).reshape(NSEL * BLOCK)
        key_live = jnp.repeat(listed, BLOCK)
        query_pos = block_id * BLOCK + offsets
        allowed = key_live[None, :] & (key_pos[None, :] <= query_pos[:, None])
        scores = jnp.einsum('thd,kd->htk', query_block, selected_keys) * score_scale
        probs = jnp.where(allowed[None], jnp.exp(scores - log_rows[block_id].T[:, :, None]), 0.0)
        reduced_probabilities = lax.optimization_barrier(probs.astype(jnp.bfloat16)).astype(jnp.float32)
        grad_value = jnp.einsum('htk,thd->kd', reduced_probabilities, grad_block)
        probability_gradient = jnp.einsum('thd,kd->htk', grad_block, selected_values)
        deltas = jnp.sum(grad_block * out_block, axis=-1).T
        score_gradient = (probs * (probability_gradient - deltas[:, :, None]) * score_scale).astype(jnp.bfloat16)
        dscores_wide = lax.optimization_barrier(score_gradient).astype(jnp.float32)
        query_gradient = jnp.einsum('htk,kd->thd', dscores_wide, selected_keys).astype(jnp.bfloat16)
        key_gradient = jnp.einsum('htk,thd->kd', dscores_wide, query_block)
        terms = jnp.concatenate([key_gradient, grad_value], axis=1).reshape(NSEL, BLOCK, 2 * HEAD_DIM)
        terms = jnp.where(listed[:, None, None], terms, 0.0)
        accumulated = accumulated.at[safe_ids].add(terms)
        return accumulated, query_gradient.reshape(BLOCK, HEADS * HEAD_DIM)

    initial = jnp.zeros((block_count, BLOCK, 2 * HEAD_DIM), jnp.float32)
    accumulated, grad_blocks = lax.scan(one_block, initial, jnp.arange(block_count, dtype=jnp.int32))
    grad_queries = grad_blocks.reshape(TOKENS, HEADS * HEAD_DIM)
    grad_keys = accumulated[:, :, :HEAD_DIM].reshape(TOKENS, HEAD_DIM)
    grad_values = accumulated[:, :, HEAD_DIM:].reshape(TOKENS, HEAD_DIM)
    weight_grad = jnp.dot(normed.T, grad_queries, preferred_element_type=jnp.float32)
    return grad_queries, grad_keys, grad_values, weight_grad
```

```python
import jax
import jax.numpy as jnp
from jax import lax
from jax.experimental import pallas as pl
from jax.experimental.pallas import tpu as pltpu
from jax.sharding import Mesh
from jax.sharding import PartitionSpec as P


BLOCK = 64
BLOCKS = 8
SLOTS = 16
PEERS = 64
ROWS = 8
TOK = 512
LANES = 128
SCALE = 0.125
KV = ("z", "y")
FAR = 1 << 20
F32 = jnp.float32
BF16 = jnp.bfloat16
VMEM = pl.BlockSpec(memory_space=pltpu.VMEM)
SMEM = pl.BlockSpec(memory_space=pltpu.SMEM)


def low_lanes(shape):
    return lax.broadcasted_iota(jnp.int32, shape, len(shape) - 1) < LANES // 2


def wanted_kernel(rank_ref, chosen_ref, out_ref):
    rank = rank_ref[0]
    peer = lax.broadcasted_iota(jnp.int32, (PEERS, SLOTS), 0)
    best = jnp.zeros((PEERS, SLOTS), jnp.int32)
    for j in range(BLOCKS):
        c = chosen_ref[j : j + 1, :]
        hit = ((c >> 3) == peer) & (c >= 0) & (peer != rank)
        best = jnp.maximum(best, jnp.where(hit, (c & 7) + 1, 0))
    best = jnp.max(best, axis=1, keepdims=True)
    out_ref[...] = jnp.broadcast_to(best, (PEERS, LANES))


def pick_kernel(asked_ref, piece_ref, out_ref):
    pieces = [piece_ref[b].astype(F32) for b in range(BLOCKS)]
    for s in range(PEERS):
        want = jnp.broadcast_to(asked_ref[s : s + 1, :], (ROWS, LANES))
        got = jnp.zeros((ROWS, LANES), F32)
        for b in range(BLOCKS):
            got = jnp.where(want == b + 1, pieces[b], got)
        out_ref[s] = got.astype(BF16)


def attend_kernel(
    slot_ref,
    rel_ref,
    fetched_ref,
    piece_ref,
    q0,
    q1,
    q2,
    q3,
    qp_ref,
    stats_ref,
    away_ref,
    own_ref,
    gq_own_ref,
    gq_far_ref,
    keys_tab,
    vals_tab,
    acc,
):
    def fill(src, at, count):
        kv = src[...].astype(F32)
        turned = pltpu.roll(kv, LANES // 2, 2)
        low = low_lanes(kv.shape)
        keys_tab[at : at + count] = jnp.where(low, kv, turned)
        vals_tab[at : at + count] = jnp.where(low, turned, kv)

    fill(fetched_ref, 0, PEERS)
    fill(piece_ref, PEERS, BLOCKS)
    acc[...] = jnp.zeros(acc.shape, F32)
    near = (q0, q1, q2, q3)
    low = low_lanes((LANES, LANES))
    row8 = lax.broadcasted_iota(jnp.int32, (ROWS, LANES), 0)
    query_t = lax.broadcasted_iota(jnp.int32, (LANES, LANES), 1) & (BLOCK - 1)

    def one_block(j, carry):
        slots = [slot_ref[j, s] for s in range(SLOTS)]
        kk = jnp.concatenate([keys_tab[i] for i in slots], axis=0)
        vv = jnp.concatenate([vals_tab[i] for i in slots], axis=0)
        k2 = jnp.concatenate([jnp.where(low, kk, 0.0), jnp.where(low, 0.0, kk)], axis=0).astype(BF16)
        v2 = jnp.concatenate([jnp.where(low, vv, 0.0), jnp.where(low, 0.0, vv)], axis=0).astype(BF16)
        at = pl.multiple_of(j * BLOCK, BLOCK)
        q = jnp.concatenate(
            [r[pl.ds(at, BLOCK), :] for r in near]
            + [qp_ref[k, pl.ds(at, BLOCK), :] for k in range(4)],
            axis=0,
        )
        g = jnp.concatenate(
            [r[pl.ds(TOK + at, BLOCK), :] for r in near]
            + [qp_ref[k, pl.ds(TOK + at, BLOCK), :] for k in range(4)],
            axis=0,
        )
        last = (((1,), (1,)), ((), ()))
        scores = lax.dot_general(k2, q, last, preferred_element_type=F32)
        dprobs = lax.dot_general(v2, g, last, preferred_element_type=F32)
        rel = jnp.concatenate([row8 + rel_ref[j, s] for s in range(SLOTS)], axis=0)
        seen = (rel <= query_t).astype(F32)
        seen = jnp.concatenate([seen] * 4, axis=1) > 0.0
        stat = stats_ref[j]
        probs = []
        dscores = []
        for h in range(2):
            s = scores[h * LANES : (h + 1) * LANES]
            d = dprobs[h * LANES : (h + 1) * LANES]
            p = jnp.where(seen, jnp.exp(s * SCALE - stat[h : h + 1, :]), 0.0)
            probs.append(p.astype(BF16))
            dscores.append((p * (d - stat[2 + h : 3 + h, :]) * SCALE).astype(BF16))
        probs = jnp.concatenate(probs, axis=0)
        dscores = jnp.concatenate(dscores, axis=0)
        plain = (((1,), (0,)), ((), ()))
        dv = lax.dot_general(probs, g, plain, preferred_element_type=F32)
        dk = lax.dot_general(dscores, q, plain, preferred_element_type=F32)
        gq = lax.dot_general(dscores, k2, (((0,), (0,)), ((), ())), preferred_element_type=F32)
        for k in range(4):
            gq_own_ref[k, pl.ds(at, BLOCK), :] = gq[k * BLOCK : (k + 1) * BLOCK]
            gq_far_ref[k, pl.ds(at, BLOCK), :] = gq[(4 + k) * BLOCK : (5 + k) * BLOCK].astype(BF16)
        both = jnp.where(low, dk[:LANES], dv[LANES:]) + pltpu.roll(
            jnp.where(low, dv[:LANES], dk[LANES:]), LANES // 2, 1
        )
        for s in range(SLOTS):
            acc[slots[s]] += both[s * ROWS : (s + 1) * ROWS]
        return carry

    lax.fori_loop(0, BLOCKS, one_block, 0)
    away_ref[...] = acc[:PEERS].astype(BF16)
    own_ref[...] = acc[PEERS:]


def settle_kernel(asked_ref, returned_ref, own_ref, out_ref):
    totals = [own_ref[b] for b in range(BLOCKS)]
    for s in range(PEERS):
        want = jnp.broadcast_to(asked_ref[s : s + 1, :], (ROWS, LANES))
        got = returned_ref[s].astype(F32)
        for b in range(BLOCKS):
            totals[b] = totals[b] + jnp.where(want == b + 1, got, 0.0)
    for b in range(BLOCKS):
        out_ref[b] = totals[b]


def place_kernel(at_ref, near_ref, far_ref, keys_ref, vals_ref):
    x = at_ref[0]
    c = at_ref[1]
    for xa in range(4):
        k = (x + 4 - xa) & 3
        for ca in range(2):
            mine = (c == ca).astype(F32)
            for b in range(BLOCKS):
                piece = near_ref[k, b] * mine + far_ref[k, b] * (1.0 - mine)
                at = b * BLOCK + (xa * 2 + ca) * ROWS
                keys_ref[at : at + ROWS, :] = piece[:, : LANES // 2]
                vals_ref[at : at + ROWS, :] = piece[:, LANES // 2 :]


def call(kernel, ins, out_shape, args, flops, **kw):
    many = isinstance(out_shape, (list, tuple))
    return pl.pallas_call(
        kernel,
        in_specs=ins,
        out_specs=[VMEM] * len(out_shape) if many else VMEM,
        out_shape=out_shape,
        cost_estimate=pl.CostEstimate(flops=flops, bytes_accessed=1 << 20, transcendentals=0),
        **kw,
    )(*args)


def sds(shape, dtype):
    return jax.ShapeDtypeStruct(shape, dtype)


def x_from(arr, k):
    return lax.ppermute(arr, "x", [(i, (i + k) % 4) for i in range(4)])


def x_back(arr, k):
    return lax.ppermute(arr, "x", [((i + k) % 4, i) for i in range(4)])


def swap(arr):
    return lax.ppermute(arr, "c", [(0, 1), (1, 0)])


def exchange(arr):
    return lax.all_to_all(arr, KV, split_axis=0, concat_axis=0, tiled=True)


def step(normed, queries, keys, values, attended, cotangent, log_sum, chosen):
    rank = lax.axis_index(KV).astype(jnp.int32)
    x = lax.axis_index("x").astype(jnp.int32)
    c = lax.axis_index("c").astype(jnp.int32)
    tp = x * 2 + c
    wanted = call(
        wanted_kernel,
        [SMEM, VMEM],
        sds((PEERS, LANES), jnp.int32),
        (rank.reshape(1), chosen),
        1 << 18,
        name="wanted",
    )
    asked = exchange(wanted)
    pairs = jnp.concatenate([keys, values], axis=1).reshape(BLOCKS, 8, ROWS, 2 * 64)
    piece = lax.dynamic_index_in_dim(pairs, tp, axis=1, keepdims=False)
    picked = call(
        pick_kernel,
        [VMEM, VMEM],
        sds((PEERS, ROWS, LANES), BF16),
        (asked, piece),
        1 << 20,
        name="pick",
    )
    fetched = exchange(picked)

    qd = jnp.concatenate([queries, cotangent], axis=0)
    deltas = jnp.sum(
        (cotangent.astype(F32) * attended.astype(F32)).reshape(TOK, 2, 64), axis=-1
    )
    stats = jnp.concatenate([log_sum.T, deltas.T], axis=0)
    qds = [qd] + [x_from(qd, k) for k in (1, 2, 3)]
    sts = [stats] + [x_from(stats, k) for k in (1, 2, 3)]
    st4 = jnp.stack(sts)
    qd_far = swap(jnp.stack(qds))
    st_far = swap(st4)
    all_stats = jnp.concatenate([st4, st_far], axis=0)
    all_stats = all_stats.reshape(8, 4, BLOCKS, BLOCK).transpose(2, 1, 0, 3).reshape(BLOCKS, 4, TOK)

    owner = chosen >> 3
    slot = jnp.where(chosen < 0, 0, jnp.where(owner == rank, PEERS + (chosen & 7), owner))
    starts = rank * TOK + jnp.arange(BLOCKS, dtype=jnp.int32)[:, None] * BLOCK
    rel = jnp.where(chosen < 0, FAR, chosen * BLOCK + ROWS * tp - starts)

    away, own, gq_own, gq_far = call(
        attend_kernel,
        [SMEM, SMEM] + [VMEM] * 8,
        [
            sds((PEERS, ROWS, LANES), BF16),
            sds((BLOCKS, ROWS, LANES), F32),
            sds((4, TOK, LANES), F32),
            sds((4, TOK, LANES), BF16),
        ],
        (slot, rel, fetched, piece, *qds, qd_far, all_stats),
        1 << 30,
        scratch_shapes=[pltpu.VMEM((PEERS + BLOCKS, ROWS, LANES), F32)] * 3,
        name="attend",
    )
    returned = exchange(away)
    gq4 = gq_own + swap(gq_far).astype(F32)
    gq = gq4[0]
    for k in (1, 2, 3):
        gq = gq + x_back(gq4[k].astype(BF16), k).astype(F32)
    grad_queries = gq.astype(BF16)
    part = lax.dot_general(
        normed, grad_queries, (((0,), (0,)), ((), ())), preferred_element_type=F32
    ).astype(BF16)
    parts = exchange(part.reshape(PEERS, 64, LANES))
    weight_grad = jnp.sum(parts.astype(F32), axis=0)

    total = call(
        settle_kernel,
        [VMEM] * 3,
        sds((BLOCKS, ROWS, LANES), F32),
        (asked, returned, own),
        1 << 20,
        name="settle",
    )
    near = jnp.stack([total] + [x_from(total, k) for k in (1, 2, 3)])
    far = swap(near)
    grad_keys, grad_values = call(
        place_kernel,
        [SMEM, VMEM, VMEM],
        [sds((TOK, 64), F32), sds((TOK, 64), F32)],
        (jnp.stack([x, c]), near, far),
        1 << 20,
        name="place",
    )
    return grad_queries, grad_keys, grad_values, weight_grad


def solution(mesh):
    torus = Mesh(mesh.devices.reshape(8, 8, 4, 2), ("z", "y", "x", "c"))
    heads = ("x", "c")
    in_specs = (
        P(KV, None),
        P(KV, heads),
        P(KV, None),
        P(KV, None),
        P(KV, heads),
        P(KV, heads),
        P(KV, heads),
        P(KV, None),
    )
    out_specs = (P(KV, heads), P(KV, None), P(KV, None), P(KV, heads))
    return jax.shard_map(step, mesh=torus, in_specs=in_specs, out_specs=out_specs, check_vma=False)
```

```python
import jax
import jax.numpy as jnp
from jax import lax
from jax.experimental import pallas as pl
from jax.experimental.pallas import tpu as pltpu
from jax.sharding import Mesh
from jax.sharding import PartitionSpec as P


BLOCK = 64
BLOCKS = 8
SLOTS = 16
PEERS = 64
ROWS = 8
TOK = 512
LANES = 128
SCALE = 0.125
KV = ("z", "y")
FAR = 1 << 20
F32 = jnp.float32
BF16 = jnp.bfloat16
VMEM = pl.BlockSpec(memory_space=pltpu.VMEM)
SMEM = pl.BlockSpec(memory_space=pltpu.SMEM)


def low_lanes(shape):
    return lax.broadcasted_iota(jnp.int32, shape, len(shape) - 1) < LANES // 2


def offer_kernel(at_ref, keys_ref, vals_ref, chosen_ref, out_ref, pairs):
    rank = at_ref[0]
    tp = at_ref[1]
    both = jnp.concatenate([keys_ref[...], vals_ref[...]], axis=0).astype(F32)
    pairs[...] = both.T
    peer = lax.broadcasted_iota(jnp.int32, (PEERS, SLOTS), 0)
    best = jnp.zeros((PEERS, SLOTS), jnp.int32)
    for j in range(BLOCKS):
        c = chosen_ref[j : j + 1, :]
        hit = ((c >> 3) == peer) & (c >= 0) & (peer != rank)
        best = jnp.maximum(best, jnp.where(hit, (c & 7) + 1, 0))
    best = jnp.max(best, axis=1, keepdims=True)
    best = jnp.broadcast_to(best, (PEERS, LANES)).astype(F32)
    pieces = []
    for b in range(BLOCKS):
        at = pl.multiple_of(b * BLOCK + tp * ROWS, ROWS)
        pieces.append(pairs[pl.ds(at, ROWS), :].astype(BF16))
    for s in range(PEERS):
        for b in range(BLOCKS):
            out_ref[s, b] = pieces[b]
        out_ref[s, BLOCKS] = jnp.broadcast_to(best[s : s + 1], (ROWS, LANES)).astype(BF16)


def pack_kernel(q_ref, g_ref, o_ref, log_ref, out_ref):
    out_ref[0:TOK] = q_ref[...]
    out_ref[TOK : 2 * TOK] = g_ref[...]
    prod = (g_ref[...].astype(F32) * o_ref[...].astype(F32)).T
    half = LANES // 2
    stats = jnp.concatenate(
        [
            log_ref[...],
            jnp.sum(prod[:half], axis=0, keepdims=True),
            jnp.sum(prod[half:], axis=0, keepdims=True),
        ],
        axis=0,
    )
    rest = jnp.concatenate([stats[:, m * LANES : (m + 1) * LANES] for m in range(4)], axis=0)
    for n in range(3):
        part = rest.astype(BF16)
        out_ref[2 * TOK + 16 * n : 2 * TOK + 16 * (n + 1)] = part
        rest = rest - part.astype(F32)


def attend_kernel(
    src_ref,
    dst_ref,
    rel_ref,
    offered_ref,
    q0,
    q1,
    q2,
    q3,
    qp_ref,
    away_ref,
    own_ref,
    gq_own_ref,
    gq_far_ref,
    stats_tab,
    acc,
):
    near = (q0, q1, q2, q3)
    acc[...] = jnp.zeros(acc.shape, F32)
    low = low_lanes((LANES, LANES))
    low4 = low_lanes((4, LANES))
    row8 = lax.broadcasted_iota(jnp.int32, (ROWS, LANES), 0)
    query_t = lax.broadcasted_iota(jnp.int32, (LANES, LANES), 1) & (BLOCK - 1)

    def stat(p):
        parts = []
        for n in range(3):
            at = 2 * TOK + 16 * n
            parts.append((near[p][at : at + 16, :] if p < 4 else qp_ref[p - 4, at : at + 16, :]).astype(F32))
        return parts[0] + parts[1] + parts[2]

    for pair in range(4):
        even, odd = stat(2 * pair), stat(2 * pair + 1)
        even_turned = pltpu.roll(even, LANES // 2, 1)
        odd_turned = pltpu.roll(odd, LANES // 2, 1)
        for j in range(BLOCKS):
            m = 4 * (j // 2)
            lo = even[m : m + 4] if j % 2 == 0 else even_turned[m : m + 4]
            hi = odd_turned[m : m + 4] if j % 2 == 0 else odd[m : m + 4]
            stats_tab[j, 0:4, pair * LANES : (pair + 1) * LANES] = jnp.where(low4, lo, hi)

    def one_block(j, carry):
        kv = jnp.concatenate([offered_ref[src_ref[j, s]].astype(F32) for s in range(SLOTS)], axis=0)
        turned = pltpu.roll(kv, LANES // 2, 1)
        k2 = jnp.concatenate([jnp.where(low, kv, 0.0), jnp.where(low, 0.0, turned)], axis=0).astype(BF16)
        v2 = jnp.concatenate([jnp.where(low, turned, 0.0), jnp.where(low, 0.0, kv)], axis=0).astype(BF16)
        at = pl.multiple_of(j * BLOCK, BLOCK)
        q = jnp.concatenate(
            [r[pl.ds(at, BLOCK), :] for r in near]
            + [qp_ref[k, pl.ds(at, BLOCK), :] for k in range(4)],
            axis=0,
        )
        g = jnp.concatenate(
            [r[pl.ds(TOK + at, BLOCK), :] for r in near]
            + [qp_ref[k, pl.ds(TOK + at, BLOCK), :] for k in range(4)],
            axis=0,
        )
        last = (((1,), (1,)), ((), ()))
        scores = lax.dot_general(k2, q, last, preferred_element_type=F32)
        dprobs = lax.dot_general(v2, g, last, preferred_element_type=F32)
        rel = jnp.concatenate([row8 + rel_ref[j, s] for s in range(SLOTS)], axis=0)
        seen = (rel <= query_t).astype(F32)
        seen = jnp.concatenate([seen] * 4, axis=1) > 0.0
        stat_j = stats_tab[j]
        probs = []
        dscores = []
        for h in range(2):
            s = scores[h * LANES : (h + 1) * LANES]
            d = dprobs[h * LANES : (h + 1) * LANES]
            p = jnp.where(seen, jnp.exp(s * SCALE - stat_j[h : h + 1, :]), 0.0)
            probs.append(p.astype(BF16))
            dscores.append((p * (d - stat_j[2 + h : 3 + h, :]) * SCALE).astype(BF16))
        probs = jnp.concatenate(probs, axis=0)
        dscores = jnp.concatenate(dscores, axis=0)
        plain = (((1,), (0,)), ((), ()))
        dv = lax.dot_general(probs, g, plain, preferred_element_type=F32)
        dk = lax.dot_general(dscores, q, plain, preferred_element_type=F32)
        gq = lax.dot_general(dscores, k2, (((0,), (0,)), ((), ())), preferred_element_type=F32)
        for k in range(4):
            gq_own_ref[k, pl.ds(at, BLOCK), :] = gq[k * BLOCK : (k + 1) * BLOCK]
            gq_far_ref[k, pl.ds(at, BLOCK), :] = gq[(4 + k) * BLOCK : (5 + k) * BLOCK].astype(BF16)
        both = jnp.where(low, dk[:LANES], dv[LANES:]) + pltpu.roll(
            jnp.where(low, dv[:LANES], dk[LANES:]), LANES // 2, 1
        )
        for s in range(SLOTS):
            acc[dst_ref[j, s]] += both[s * ROWS : (s + 1) * ROWS]
        return carry

    lax.fori_loop(0, BLOCKS, one_block, 0)
    away_ref[...] = acc[:PEERS].astype(BF16)
    own_ref[...] = acc[PEERS:]


def settle_kernel(asked_ref, returned_ref, own_ref, out_ref):
    totals = [own_ref[b] for b in range(BLOCKS)]
    for s in range(PEERS):
        want = asked_ref[s].astype(F32)
        got = returned_ref[s].astype(F32)
        for b in range(BLOCKS):
            totals[b] = totals[b] + jnp.where(want == b + 1.0, got, 0.0)
    for b in range(BLOCKS):
        out_ref[b] = totals[b]


def place_kernel(at_ref, near_ref, far_ref, keys_ref, vals_ref, rows):
    x = at_ref[0]
    mine = jnp.full((ROWS, LANES), at_ref[1], jnp.int32)
    for xa in range(4):
        k = (x + 4 - xa) & 3
        for ca in range(2):
            for b in range(BLOCKS):
                at = b * BLOCK + (xa * 2 + ca) * ROWS
                rows[at : at + ROWS, :] = jnp.where(mine == ca, near_ref[k, b], far_ref[k, b])
    turned = rows[...].T
    keys_ref[...] = turned[: LANES // 2]
    vals_ref[...] = turned[LANES // 2 :]


def call(kernel, ins, out_shape, args, flops, **kw):
    many = isinstance(out_shape, (list, tuple))
    return pl.pallas_call(
        kernel,
        in_specs=ins,
        out_specs=[VMEM] * len(out_shape) if many else VMEM,
        out_shape=out_shape,
        cost_estimate=pl.CostEstimate(flops=flops, bytes_accessed=1 << 20, transcendentals=0),
        **kw,
    )(*args)


def sds(shape, dtype):
    return jax.ShapeDtypeStruct(shape, dtype)


def x_from(arr, k):
    return lax.ppermute(arr, "x", [(i, (i + k) % 4) for i in range(4)])


def x_back(arr, k):
    return lax.ppermute(arr, "x", [((i + k) % 4, i) for i in range(4)])


def swap(arr):
    return lax.ppermute(arr, "c", [(0, 1), (1, 0)])


def exchange(arr):
    return lax.all_to_all(arr, KV, split_axis=0, concat_axis=0, tiled=True)


def step(normed, queries, keys, values, attended, cotangent, log_sum, chosen):
    rank = lax.axis_index(KV).astype(jnp.int32)
    x = lax.axis_index("x").astype(jnp.int32)
    c = lax.axis_index("c").astype(jnp.int32)
    tp = x * 2 + c
    offer = call(
        offer_kernel,
        [SMEM] + [VMEM] * 3,
        sds((PEERS, BLOCKS + 1, ROWS, LANES), BF16),
        (jnp.stack([rank, tp]), keys.T, values.T, chosen),
        1 << 18,
        scratch_shapes=[pltpu.VMEM((TOK, LANES), F32)],
        name="offer",
    )
    offered = exchange(offer)
    asked = offered[:, BLOCKS]

    qd = call(
        pack_kernel,
        [VMEM] * 4,
        sds((2 * TOK + 48, LANES), BF16),
        (queries, cotangent, attended, log_sum.T),
        1 << 18,
        name="pack",
    )
    qds = [qd] + [x_from(qd, k) for k in (1, 2, 3)]
    qd_far = swap(jnp.stack(qds))

    owner = chosen >> 3
    inner = chosen & 7
    listed = chosen >= 0
    src = jnp.where(listed, owner * (BLOCKS + 1) + inner, 0)
    dst = jnp.where(listed, jnp.where(owner == rank, PEERS + inner, owner), 0)
    starts = rank * TOK + lax.broadcasted_iota(jnp.int32, chosen.shape, 0) * BLOCK
    rel = jnp.where(listed, chosen * BLOCK + ROWS * tp - starts, FAR)

    away, own, gq_own, gq_far = call(
        attend_kernel,
        [SMEM] * 3 + [VMEM] * 6,
        [
            sds((PEERS, ROWS, LANES), BF16),
            sds((BLOCKS, ROWS, LANES), F32),
            sds((4, TOK, LANES), F32),
            sds((4, TOK, LANES), BF16),
        ],
        (src, dst, rel, offered.reshape(PEERS * (BLOCKS + 1), ROWS, LANES), *qds, qd_far),
        1 << 30,
        scratch_shapes=[
            pltpu.VMEM((BLOCKS, 8, TOK), F32),
            pltpu.VMEM((PEERS + BLOCKS, ROWS, LANES), F32),
        ],
        name="attend",
    )
    gq4 = gq_own + swap(gq_far).astype(F32)
    returned = exchange(away)
    gq = gq4[0]
    for k in (1, 2, 3):
        gq = gq + x_back(gq4[k].astype(BF16), k).astype(F32)
    grad_queries = gq.astype(BF16)
    part = lax.dot_general(
        normed, grad_queries, (((0,), (0,)), ((), ())), preferred_element_type=F32
    ).astype(BF16)
    parts = exchange(part.reshape(PEERS, 64, LANES))
    weight_grad = jnp.sum(parts.astype(F32), axis=0)

    total = call(
        settle_kernel,
        [VMEM] * 3,
        sds((BLOCKS, ROWS, LANES), F32),
        (asked, returned, own),
        1 << 20,
        name="settle",
    )
    near = jnp.stack([total] + [x_from(total, k) for k in (1, 2, 3)])
    far = swap(near)
    grad_keys, grad_values = call(
        place_kernel,
        [SMEM, VMEM, VMEM],
        [sds((64, TOK), F32), sds((64, TOK), F32)],
        (jnp.stack([x, c]), near, far),
        1 << 20,
        scratch_shapes=[pltpu.VMEM((TOK, LANES), F32)],
        name="place",
    )
    return grad_queries, grad_keys.T, grad_values.T, weight_grad


def solution(mesh):
    torus = Mesh(mesh.devices.reshape(8, 8, 4, 2), ("z", "y", "x", "c"))
    heads = ("x", "c")
    in_specs = (
        P(KV, None),
        P(KV, heads),
        P(KV, None),
        P(KV, None),
        P(KV, heads),
        P(KV, heads),
        P(KV, heads),
        P(KV, None),
    )
    out_specs = (P(KV, heads), P(KV, None), P(KV, None), P(KV, heads))
    return jax.shard_map(step, mesh=torus, in_specs=in_specs, out_specs=out_specs, check_vma=False)
```

```python
import jax
import jax.numpy as jnp
from jax import lax
from jax.experimental import pallas as pl
from jax.experimental.pallas import tpu as pltpu
from jax.sharding import Mesh
from jax.sharding import PartitionSpec as P


BLOCK = 64
BLOCKS = 8
SLOTS = 16
PEERS = 64
SIDE = 8
ROWS = 8
TOK = 512
LANES = 128
SCALE = 0.125
KV = ("z", "y")
ALL = ("z", "y", "x", "c")
FAR = 1 << 20
F32 = jnp.float32
BF16 = jnp.bfloat16
VMEM = pl.BlockSpec(memory_space=pltpu.VMEM)
SMEM = pl.BlockSpec(memory_space=pltpu.SMEM)


def low_lanes(shape):
    return lax.broadcasted_iota(jnp.int32, shape, len(shape) - 1) < LANES // 2


def offer_kernel(at_ref, keys_ref, vals_ref, chosen_ref, out_ref, piece_ref, pairs):
    rank = at_ref[0]
    tp = at_ref[1]
    flip = at_ref[2]
    both = jnp.concatenate([keys_ref[...], vals_ref[...]], axis=0).astype(F32)
    pairs[...] = both.T
    at = lax.broadcasted_iota(jnp.int32, (PEERS, SLOTS), 0)
    peer = jnp.where(jnp.full(at.shape, flip, jnp.int32) == 0, at, (at & 7) * 8 + (at >> 3))
    best = jnp.zeros((PEERS, SLOTS), jnp.int32)
    for j in range(BLOCKS):
        c = chosen_ref[j : j + 1, :]
        hit = ((c >> 3) == peer) & (c >= 0) & (peer != rank)
        best = jnp.maximum(best, jnp.where(hit, (c & 7) + 1, 0))
    best = jnp.max(best, axis=1, keepdims=True)
    best = jnp.broadcast_to(best, (PEERS, LANES)).astype(F32)
    for b in range(BLOCKS):
        at = pl.multiple_of(b * BLOCK + tp * ROWS, ROWS)
        piece = pairs[pl.ds(at, ROWS), :].astype(BF16)
        piece_ref[b] = piece
        for i in range(SIDE):
            out_ref[i, b] = piece
    for i in range(SIDE):
        out_ref[i, BLOCKS] = best[i * SIDE : (i + 1) * SIDE].astype(BF16)


def pick_kernel(wants_ref, pushed_ref, out_ref):
    for r in range(SIDE):
        pieces = [pushed_ref[r, b].astype(F32) for b in range(BLOCKS)]
        for i in range(SIDE):
            want = jnp.broadcast_to(wants_ref[i].astype(F32)[r : r + 1], (ROWS, LANES))
            got = jnp.zeros((ROWS, LANES), F32)
            for b in range(BLOCKS):
                got = jnp.where(want == b + 1.0, pieces[b], got)
            out_ref[i, r] = got.astype(BF16)


def relay_kernel(wants_ref, given_ref, out_ref):
    for r in range(SIDE):
        totals = [jnp.zeros((ROWS, LANES), F32) for _ in range(BLOCKS)]
        for i in range(SIDE):
            want = jnp.broadcast_to(wants_ref[i].astype(F32)[r : r + 1], (ROWS, LANES))
            got = given_ref[i, r].astype(F32)
            for b in range(BLOCKS):
                totals[b] = totals[b] + jnp.where(want == b + 1.0, got, 0.0)
        for b in range(BLOCKS):
            out_ref[r, b] = totals[b].astype(BF16)


def settle_kernel(own_ref, given_ref, out_ref):
    for b in range(BLOCKS):
        total = own_ref[b]
        for i in range(SIDE):
            total = total + given_ref[i, b].astype(F32)
        out_ref[b] = total


def weight_kernel(at_ref, grad_ref, normed_ref, out_ref, grad_t):
    i = pl.program_id(0)
    flip = at_ref[2]

    @pl.when(i == 0)
    def _():
        grad_t[...] = grad_ref[...].astype(F32).T.astype(BF16)

    part = lax.dot_general(
        grad_t[...], normed_ref[...], (((1,), (0,)), ((), ())), preferred_element_type=F32
    )
    part = part.T.astype(BF16)
    for n in range(SIDE):
        at = jnp.where(flip == 0, i * SIDE + n, n * SIDE + i)
        out_ref[at] = part[n * BLOCK : (n + 1) * BLOCK]


def pack_kernel(q_ref, g_ref, o_ref, log_ref, out_ref):
    out_ref[0:TOK] = q_ref[...]
    out_ref[TOK : 2 * TOK] = g_ref[...]
    prod = (g_ref[...].astype(F32) * o_ref[...].astype(F32)).T
    half = LANES // 2
    stats = jnp.concatenate(
        [
            log_ref[...],
            jnp.sum(prod[:half], axis=0, keepdims=True),
            jnp.sum(prod[half:], axis=0, keepdims=True),
        ],
        axis=0,
    )
    rest = jnp.concatenate([stats[:, m * LANES : (m + 1) * LANES] for m in range(4)], axis=0)
    for n in range(3):
        part = rest.astype(BF16)
        out_ref[2 * TOK + 16 * n : 2 * TOK + 16 * (n + 1)] = part
        rest = rest - part.astype(F32)


def attend_kernel(
    slot_ref,
    rel_ref,
    fetched_ref,
    piece_ref,
    q0,
    q1,
    q2,
    q3,
    qp_ref,
    away_ref,
    own_ref,
    gq_own_ref,
    gq_far_ref,
    stats_tab,
    table,
    acc,
):
    near = (q0, q1, q2, q3)
    table[:PEERS] = fetched_ref[...].astype(F32)
    table[PEERS:] = piece_ref[...].astype(F32)
    acc[...] = jnp.zeros(acc.shape, F32)
    low = low_lanes((LANES, LANES))
    low4 = low_lanes((4, LANES))
    row8 = lax.broadcasted_iota(jnp.int32, (ROWS, LANES), 0)
    query_t = lax.broadcasted_iota(jnp.int32, (LANES, LANES), 1) & (BLOCK - 1)

    def stat(p):
        parts = []
        for n in range(3):
            at = 2 * TOK + 16 * n
            parts.append((near[p][at : at + 16, :] if p < 4 else qp_ref[p - 4, at : at + 16, :]).astype(F32))
        return parts[0] + parts[1] + parts[2]

    for pair in range(4):
        even, odd = stat(2 * pair), stat(2 * pair + 1)
        even_turned = pltpu.roll(even, LANES // 2, 1)
        odd_turned = pltpu.roll(odd, LANES // 2, 1)
        for j in range(BLOCKS):
            m = 4 * (j // 2)
            lo = even[m : m + 4] if j % 2 == 0 else even_turned[m : m + 4]
            hi = odd_turned[m : m + 4] if j % 2 == 0 else odd[m : m + 4]
            stats_tab[j, 0:4, pair * LANES : (pair + 1) * LANES] = jnp.where(low4, lo, hi)

    def one_block(j, carry):
        kv = jnp.concatenate([table[slot_ref[j, s]] for s in range(SLOTS)], axis=0)
        turned = pltpu.roll(kv, LANES // 2, 1)
        k2 = jnp.concatenate([jnp.where(low, kv, 0.0), jnp.where(low, 0.0, turned)], axis=0).astype(BF16)
        v2 = jnp.concatenate([jnp.where(low, turned, 0.0), jnp.where(low, 0.0, kv)], axis=0).astype(BF16)
        at = pl.multiple_of(j * BLOCK, BLOCK)
        q = jnp.concatenate(
            [r[pl.ds(at, BLOCK), :] for r in near]
            + [qp_ref[k, pl.ds(at, BLOCK), :] for k in range(4)],
            axis=0,
        )
        g = jnp.concatenate(
            [r[pl.ds(TOK + at, BLOCK), :] for r in near]
            + [qp_ref[k, pl.ds(TOK + at, BLOCK), :] for k in range(4)],
            axis=0,
        )
        last = (((1,), (1,)), ((), ()))
        scores = lax.dot_general(k2, q, last, preferred_element_type=F32)
        dprobs = lax.dot_general(v2, g, last, preferred_element_type=F32)
        rel = jnp.concatenate([row8 + rel_ref[j, s] for s in range(SLOTS)], axis=0)
        seen = (rel <= query_t).astype(F32)
        seen = jnp.concatenate([seen] * 4, axis=1) > 0.0
        stat_j = stats_tab[j]
        probs = []
        dscores = []
        for h in range(2):
            s = scores[h * LANES : (h + 1) * LANES]
            d = dprobs[h * LANES : (h + 1) * LANES]
            p = jnp.where(seen, jnp.exp(s * SCALE - stat_j[h : h + 1, :]), 0.0)
            probs.append(p.astype(BF16))
            dscores.append((p * (d - stat_j[2 + h : 3 + h, :]) * SCALE).astype(BF16))
        probs = jnp.concatenate(probs, axis=0)
        dscores = jnp.concatenate(dscores, axis=0)
        plain = (((1,), (0,)), ((), ()))
        dv = lax.dot_general(probs, g, plain, preferred_element_type=F32)
        dk = lax.dot_general(dscores, q, plain, preferred_element_type=F32)
        gq = lax.dot_general(dscores, k2, (((0,), (0,)), ((), ())), preferred_element_type=F32)
        for k in range(4):
            gq_own_ref[k, pl.ds(at, BLOCK), :] = gq[k * BLOCK : (k + 1) * BLOCK]
            gq_far_ref[k, pl.ds(at, BLOCK), :] = gq[(4 + k) * BLOCK : (5 + k) * BLOCK].astype(BF16)
        both = jnp.where(low, dk[:LANES], dv[LANES:]) + pltpu.roll(
            jnp.where(low, dv[:LANES], dk[LANES:]), LANES // 2, 1
        )
        for s in range(SLOTS):
            acc[slot_ref[j, s]] += both[s * ROWS : (s + 1) * ROWS]
        return carry

    lax.fori_loop(0, BLOCKS, one_block, 0)
    away_ref[...] = acc[:PEERS].astype(BF16)
    own_ref[...] = acc[PEERS:]


def place_kernel(at_ref, near_ref, far_ref, keys_ref, vals_ref, rows):
    x = at_ref[0]
    mine = jnp.full((ROWS, LANES), at_ref[1], jnp.int32)
    for xa in range(4):
        k = (x + 4 - xa) & 3
        for ca in range(2):
            for b in range(BLOCKS):
                at = b * BLOCK + (xa * 2 + ca) * ROWS
                rows[at : at + ROWS, :] = jnp.where(mine == ca, near_ref[k, b], far_ref[k, b])
    turned = rows[...].T
    keys_ref[...] = turned[: LANES // 2]
    vals_ref[...] = turned[LANES // 2 :]


def call(kernel, ins, out_shape, args, flops, **kw):
    many = isinstance(out_shape, (list, tuple))
    return pl.pallas_call(
        kernel,
        in_specs=ins,
        out_specs=[VMEM] * len(out_shape) if many else VMEM,
        out_shape=out_shape,
        cost_estimate=pl.CostEstimate(flops=flops, bytes_accessed=1 << 20, transcendentals=0),
        **kw,
    )(*args)


def sds(shape, dtype):
    return jax.ShapeDtypeStruct(shape, dtype)


def x_from(arr, k):
    return lax.ppermute(arr, "x", [(i, (i + k) % 4) for i in range(4)])


def x_back(arr, k):
    return lax.ppermute(arr, "x", [((i + k) % 4, i) for i in range(4)])


def swap(arr):
    return lax.ppermute(arr, "c", [(0, 1), (1, 0)])


def device(z, y, x, c):
    return ((z * 8 + y) * 4 + x) * 2 + c


def lines(first):
    out = []
    for x in range(4):
        for c in range(2):
            for a in range(SIDE):
                if (c == 0) == first:
                    out.append([device(i, a, x, c) for i in range(SIDE)])
                else:
                    out.append([device(a, i, x, c) for i in range(SIDE)])
    return out


def along(arr, first):
    return lax.all_to_all(
        arr, ALL, split_axis=0, concat_axis=0, tiled=True, axis_index_groups=lines(first)
    )


def step(normed, queries, keys, values, attended, cotangent, log_sum, chosen):
    rank = lax.axis_index(KV).astype(jnp.int32)
    x = lax.axis_index("x").astype(jnp.int32)
    c = lax.axis_index("c").astype(jnp.int32)
    tp = x * 2 + c
    spot = jnp.stack([rank, tp, c])
    offer, piece = call(
        offer_kernel,
        [SMEM] + [VMEM] * 3,
        [
            sds((SIDE, BLOCKS + 1, ROWS, LANES), BF16),
            sds((BLOCKS, ROWS, LANES), BF16),
        ],
        (spot, keys.T, values.T, chosen),
        1 << 18,
        scratch_shapes=[pltpu.VMEM((TOK, LANES), F32)],
        name="offer",
    )
    pushed = along(offer, True)
    wants = swap(pushed[:, BLOCKS])
    picked = call(
        pick_kernel,
        [VMEM] * 2,
        sds((SIDE, SIDE, ROWS, LANES), BF16),
        (wants, pushed),
        1 << 20,
        name="pick",
    )
    fetched = along(picked, False).reshape(PEERS, ROWS, LANES)

    qd = call(
        pack_kernel,
        [VMEM] * 4,
        sds((2 * TOK + 48, LANES), BF16),
        (queries, cotangent, attended, log_sum.T),
        1 << 18,
        name="pack",
    )
    qds = [qd] + [x_from(qd, k) for k in (1, 2, 3)]
    qd_far = swap(jnp.stack(qds))

    owner = chosen >> 3
    inner = chosen & 7
    listed = chosen >= 0
    peer = jnp.where(c == 0, (owner & 7) * 8 + (owner >> 3), owner)
    slot = jnp.where(listed, jnp.where(owner == rank, PEERS + inner, peer), 0)
    starts = rank * TOK + lax.broadcasted_iota(jnp.int32, chosen.shape, 0) * BLOCK
    rel = jnp.where(listed, chosen * BLOCK + ROWS * tp - starts, FAR)

    away, own, gq_own, gq_far = call(
        attend_kernel,
        [SMEM] * 2 + [VMEM] * 7,
        [
            sds((PEERS, ROWS, LANES), BF16),
            sds((BLOCKS, ROWS, LANES), F32),
            sds((4, TOK, LANES), F32),
            sds((4, TOK, LANES), BF16),
        ],
        (slot, rel, fetched, piece, *qds, qd_far),
        1 << 30,
        scratch_shapes=[
            pltpu.VMEM((BLOCKS, 8, TOK), F32),
            pltpu.VMEM((PEERS + BLOCKS, ROWS, LANES), F32),
            pltpu.VMEM((PEERS + BLOCKS, ROWS, LANES), F32),
        ],
        name="attend",
    )
    gq4 = gq_own + swap(gq_far).astype(F32)
    given = along(away.reshape(SIDE, SIDE, ROWS, LANES), False)
    relayed = call(
        relay_kernel,
        [VMEM] * 2,
        sds((SIDE, BLOCKS, ROWS, LANES), BF16),
        (wants, given),
        1 << 20,
        name="relay",
    )
    returned = along(relayed, True)
    gq = gq4[0]
    for k in (1, 2, 3):
        gq = gq + x_back(gq4[k].astype(BF16), k).astype(F32)
    grad_queries = gq.astype(BF16)
    part = pl.pallas_call(
        weight_kernel,
        grid=(SIDE,),
        in_specs=[
            SMEM,
            pl.BlockSpec((TOK, LANES), lambda i: (0, 0)),
            pl.BlockSpec((TOK, TOK), lambda i: (0, i)),
        ],
        out_specs=pl.BlockSpec((PEERS, BLOCK, LANES), lambda i: (0, 0, 0)),
        out_shape=sds((PEERS, BLOCK, LANES), BF16),
        scratch_shapes=[pltpu.VMEM((LANES, TOK), BF16)],
        cost_estimate=pl.CostEstimate(flops=1 << 29, bytes_accessed=5 << 20, transcendentals=0),
        name="product",
    )(spot, grad_queries, normed)
    parts = along(part.reshape(SIDE, SIDE, BLOCK, LANES), True)
    half = jnp.sum(parts.astype(F32), axis=0).astype(BF16)
    parts = along(half, False)
    weight_grad = jnp.sum(parts.astype(F32), axis=0)

    total = call(
        settle_kernel,
        [VMEM] * 2,
        sds((BLOCKS, ROWS, LANES), F32),
        (own, returned),
        1 << 20,
        name="settle",
    )
    near = jnp.stack([total] + [x_from(total, k) for k in (1, 2, 3)])
    far = swap(near)
    grad_keys, grad_values = call(
        place_kernel,
        [SMEM, VMEM, VMEM],
        [sds((64, TOK), F32), sds((64, TOK), F32)],
        (jnp.stack([x, c]), near, far),
        1 << 20,
        scratch_shapes=[pltpu.VMEM((TOK, LANES), F32)],
        name="place",
    )
    return grad_queries, grad_keys.T, grad_values.T, weight_grad


def solution(mesh):
    torus = Mesh(mesh.devices.reshape(8, 8, 4, 2), ("z", "y", "x", "c"))
    heads = ("x", "c")
    in_specs = (
        P(KV, None),
        P(KV, heads),
        P(KV, None),
        P(KV, None),
        P(KV, heads),
        P(KV, heads),
        P(KV, heads),
        P(KV, None),
    )
    out_specs = (P(KV, heads), P(KV, None), P(KV, None), P(KV, heads))
    return jax.shard_map(step, mesh=torus, in_specs=in_specs, out_specs=out_specs, check_vma=False)
```

```python
import jax
import jax.numpy as jnp
from jax import lax
from jax.experimental import pallas as pl
from jax.experimental.pallas import tpu as pltpu
from jax.sharding import Mesh
from jax.sharding import PartitionSpec as P


BLOCK = 64
BLOCKS = 8
SLOTS = 16
PEERS = 64
SIDE = 8
ROWS = 8
TOK = 512
LANES = 128
SCALE = 0.125
KV = ("z", "y")
ALL = ("z", "y", "x", "c")
FAR = 1 << 20
F32 = jnp.float32
BF16 = jnp.bfloat16
VMEM = pl.BlockSpec(memory_space=pltpu.VMEM)
SMEM = pl.BlockSpec(memory_space=pltpu.SMEM)


def low_lanes(shape):
    return lax.broadcasted_iota(jnp.int32, shape, len(shape) - 1) < LANES // 2


def offer_kernel(rank_ref, tp_ref, keys_ref, vals_ref, chosen_ref, out_ref, piece_ref, pairs):
    rank = rank_ref[0]
    tp = tp_ref[0]
    flip = tp & 1
    both = jnp.concatenate([keys_ref[...], vals_ref[...]], axis=0).astype(F32)
    pairs[...] = both.T
    at = lax.broadcasted_iota(jnp.int32, (PEERS, SLOTS), 0)
    peer = jnp.where(jnp.full(at.shape, flip, jnp.int32) == 0, at, (at & 7) * 8 + (at >> 3))
    best = jnp.zeros((PEERS, SLOTS), jnp.int32)
    for j in range(BLOCKS):
        c = chosen_ref[j : j + 1, :]
        hit = ((c >> 3) == peer) & (c >= 0) & (peer != rank)
        best = jnp.maximum(best, jnp.where(hit, (c & 7) + 1, 0))
    best = jnp.max(best, axis=1, keepdims=True)
    best = jnp.broadcast_to(best, (PEERS, LANES)).astype(F32)
    for b in range(BLOCKS):
        at = pl.multiple_of(b * BLOCK + tp * ROWS, ROWS)
        piece = pairs[pl.ds(at, ROWS), :].astype(BF16)
        piece_ref[b] = piece
        for i in range(SIDE):
            out_ref[i, b] = piece
    for i in range(SIDE):
        out_ref[i, BLOCKS] = best[i * SIDE : (i + 1) * SIDE].astype(BF16)


def pick_kernel(wants_ref, pushed_ref, out_ref):
    for r in range(SIDE):
        pieces = [pushed_ref[r, b].astype(F32) for b in range(BLOCKS)]
        for i in range(SIDE):
            want = jnp.broadcast_to(wants_ref[i].astype(F32)[r : r + 1], (ROWS, LANES))
            got = jnp.zeros((ROWS, LANES), F32)
            for b in range(BLOCKS):
                got = jnp.where(want == b + 1.0, pieces[b], got)
            out_ref[i, r] = got.astype(BF16)


def relay_kernel(wants_ref, given_ref, out_ref):
    for r in range(SIDE):
        totals = [jnp.zeros((ROWS, LANES), F32) for _ in range(BLOCKS)]
        for i in range(SIDE):
            want = jnp.broadcast_to(wants_ref[i].astype(F32)[r : r + 1], (ROWS, LANES))
            got = given_ref[i, r].astype(F32)
            for b in range(BLOCKS):
                totals[b] = totals[b] + jnp.where(want == b + 1.0, got, 0.0)
        for b in range(BLOCKS):
            out_ref[r, b] = totals[b].astype(BF16)


def settle_kernel(own_ref, given_ref, out_ref):
    for b in range(BLOCKS):
        total = own_ref[b]
        for i in range(SIDE):
            total = total + given_ref[i, b].astype(F32)
        out_ref[b] = total


def pack_kernel(q_ref, g_ref, o_ref, log_ref, out_ref):
    out_ref[0:TOK] = q_ref[...]
    out_ref[TOK : 2 * TOK] = g_ref[...]
    prod = (g_ref[...].astype(F32) * o_ref[...].astype(F32)).T
    half = LANES // 2
    stats = jnp.concatenate(
        [
            log_ref[...],
            jnp.sum(prod[:half], axis=0, keepdims=True),
            jnp.sum(prod[half:], axis=0, keepdims=True),
        ],
        axis=0,
    )
    rest = jnp.concatenate([stats[:, m * LANES : (m + 1) * LANES] for m in range(4)], axis=0)
    for n in range(3):
        part = rest.astype(BF16)
        out_ref[2 * TOK + 16 * n : 2 * TOK + 16 * (n + 1)] = part
        rest = rest - part.astype(F32)


def attend_kernel(
    slot_ref,
    rel_ref,
    fetched_ref,
    piece_ref,
    q0,
    q1,
    q2,
    q3,
    qp_ref,
    away_ref,
    own_ref,
    gq_own_ref,
    gq_far_ref,
    stats_tab,
    table,
    acc,
):
    near = (q0, q1, q2, q3)
    table[:PEERS] = fetched_ref[...].astype(F32)
    table[PEERS:] = piece_ref[...].astype(F32)
    acc[...] = jnp.zeros(acc.shape, F32)
    low = low_lanes((LANES, LANES))
    low4 = low_lanes((4, LANES))
    row8 = lax.broadcasted_iota(jnp.int32, (ROWS, LANES), 0)
    query_t = lax.broadcasted_iota(jnp.int32, (LANES, LANES), 1) & (BLOCK - 1)

    def stat(p):
        parts = []
        for n in range(3):
            at = 2 * TOK + 16 * n
            parts.append((near[p][at : at + 16, :] if p < 4 else qp_ref[p - 4, at : at + 16, :]).astype(F32))
        return parts[0] + parts[1] + parts[2]

    for pair in range(4):
        even, odd = stat(2 * pair), stat(2 * pair + 1)
        even_turned = pltpu.roll(even, LANES // 2, 1)
        odd_turned = pltpu.roll(odd, LANES // 2, 1)
        for j in range(BLOCKS):
            m = 4 * (j // 2)
            lo = even[m : m + 4] if j % 2 == 0 else even_turned[m : m + 4]
            hi = odd_turned[m : m + 4] if j % 2 == 0 else odd[m : m + 4]
            stats_tab[j, 0:4, pair * LANES : (pair + 1) * LANES] = jnp.where(low4, lo, hi)

    def one_block(j, carry):
        kv = jnp.concatenate([table[slot_ref[j, s]] for s in range(SLOTS)], axis=0)
        turned = pltpu.roll(kv, LANES // 2, 1)
        k2 = jnp.concatenate([jnp.where(low, kv, 0.0), jnp.where(low, 0.0, turned)], axis=0).astype(BF16)
        v2 = jnp.concatenate([jnp.where(low, turned, 0.0), jnp.where(low, 0.0, kv)], axis=0).astype(BF16)
        at = pl.multiple_of(j * BLOCK, BLOCK)
        q = jnp.concatenate(
            [r[pl.ds(at, BLOCK), :] for r in near]
            + [qp_ref[k, pl.ds(at, BLOCK), :] for k in range(4)],
            axis=0,
        )
        g = jnp.concatenate(
            [r[pl.ds(TOK + at, BLOCK), :] for r in near]
            + [qp_ref[k, pl.ds(TOK + at, BLOCK), :] for k in range(4)],
            axis=0,
        )
        last = (((1,), (1,)), ((), ()))
        scores = lax.dot_general(k2, q, last, preferred_element_type=F32)
        dprobs = lax.dot_general(v2, g, last, preferred_element_type=F32)
        rel = jnp.concatenate([row8 + rel_ref[j, s] for s in range(SLOTS)], axis=0)
        seen = (rel <= query_t).astype(F32)
        seen = jnp.concatenate([seen] * 4, axis=1) > 0.0
        stat_j = stats_tab[j]
        probs = []
        dscores = []
        for h in range(2):
            s = scores[h * LANES : (h + 1) * LANES]
            d = dprobs[h * LANES : (h + 1) * LANES]
            p = jnp.where(seen, jnp.exp(s * SCALE - stat_j[h : h + 1, :]), 0.0)
            probs.append(p.astype(BF16))
            dscores.append((p * (d - stat_j[2 + h : 3 + h, :]) * SCALE).astype(BF16))
        probs = jnp.concatenate(probs, axis=0)
        dscores = jnp.concatenate(dscores, axis=0)
        plain = (((1,), (0,)), ((), ()))
        dv = lax.dot_general(probs, g, plain, preferred_element_type=F32)
        dk = lax.dot_general(dscores, q, plain, preferred_element_type=F32)
        gq = lax.dot_general(dscores, k2, (((0,), (0,)), ((), ())), preferred_element_type=F32)
        for k in range(4):
            gq_own_ref[k, pl.ds(at, BLOCK), :] = gq[k * BLOCK : (k + 1) * BLOCK]
            gq_far_ref[k, pl.ds(at, BLOCK), :] = gq[(4 + k) * BLOCK : (5 + k) * BLOCK].astype(BF16)
        both = jnp.where(low, dk[:LANES], dv[LANES:]) + pltpu.roll(
            jnp.where(low, dv[:LANES], dk[LANES:]), LANES // 2, 1
        )
        for s in range(SLOTS):
            acc[slot_ref[j, s]] += both[s * ROWS : (s + 1) * ROWS]
        return carry

    lax.fori_loop(0, BLOCKS, one_block, 0)
    away_ref[...] = acc[:PEERS].astype(BF16)
    own_ref[...] = acc[PEERS:]


def place_kernel(tp_ref, near_ref, far_ref, keys_ref, vals_ref, rows):
    x = tp_ref[0] >> 1
    mine = jnp.full((ROWS, LANES), tp_ref[0] & 1, jnp.int32)
    for xa in range(4):
        k = (x + 4 - xa) & 3
        for ca in range(2):
            for b in range(BLOCKS):
                at = b * BLOCK + (xa * 2 + ca) * ROWS
                rows[at : at + ROWS, :] = jnp.where(mine == ca, near_ref[k, b], far_ref[k, b])
    turned = rows[...].T
    keys_ref[...] = turned[: LANES // 2]
    vals_ref[...] = turned[LANES // 2 :]


def call(kernel, ins, out_shape, args, flops, **kw):
    many = isinstance(out_shape, (list, tuple))
    return pl.pallas_call(
        kernel,
        in_specs=ins,
        out_specs=[VMEM] * len(out_shape) if many else VMEM,
        out_shape=out_shape,
        cost_estimate=pl.CostEstimate(flops=flops, bytes_accessed=1 << 20, transcendentals=0),
        compiler_params=pltpu.CompilerParams(vmem_limit_bytes=24 << 20),
        **kw,
    )(*args)


def sds(shape, dtype):
    return jax.ShapeDtypeStruct(shape, dtype)


def held(shape, dtype):
    return pltpu.VMEM(shape, dtype)


def x_from(arr, k):
    return lax.ppermute(arr, "x", [(i, (i + k) % 4) for i in range(4)])


def x_back(arr, k):
    return lax.ppermute(arr, "x", [((i + k) % 4, i) for i in range(4)])


def swap(arr):
    return lax.ppermute(arr, "c", [(0, 1), (1, 0)])


def device(z, y, x, c):
    return ((z * 8 + y) * 4 + x) * 2 + c


def lines(first):
    out = []
    for x in range(4):
        for c in range(2):
            for a in range(SIDE):
                if (c == 0) == first:
                    out.append([device(i, a, x, c) for i in range(SIDE)])
                else:
                    out.append([device(a, i, x, c) for i in range(SIDE)])
    return out


def along(arr, first):
    return lax.all_to_all(
        arr, ALL, split_axis=0, concat_axis=0, tiled=True, axis_index_groups=lines(first)
    )


def exchange(arr):
    return lax.all_to_all(arr, KV, split_axis=0, concat_axis=0, tiled=True)


def near_core(arr):
    return pltpu.with_memory_space_constraint(arr, pltpu.VMEM)


def step(normed, queries, keys, values, attended, cotangent, log_sum, chosen):
    rank = lax.axis_index(KV).astype(jnp.int32)
    x = lax.axis_index("x").astype(jnp.int32)
    c = lax.axis_index("c").astype(jnp.int32)
    tp = x * 2 + c
    offer, piece = call(
        offer_kernel,
        [SMEM] * 2 + [VMEM] * 3,
        [
            held((SIDE, BLOCKS + 1, ROWS, LANES), BF16),
            held((BLOCKS, ROWS, LANES), BF16),
        ],
        (rank.reshape(1), tp.reshape(1), keys.T, values.T, chosen),
        1 << 18,
        scratch_shapes=[pltpu.VMEM((TOK, LANES), F32)],
        name="offer",
    )
    pushed = along(offer, True)
    wants = swap(pushed[:, BLOCKS])
    picked = call(
        pick_kernel,
        [VMEM] * 2,
        held((SIDE, SIDE, ROWS, LANES), BF16),
        (near_core(wants), near_core(pushed)),
        1 << 20,
        name="pick",
    )
    fetched = along(picked, False).reshape(PEERS, ROWS, LANES)

    qd = call(
        pack_kernel,
        [VMEM] * 4,
        held((2 * TOK + 48, LANES), BF16),
        (queries, cotangent, attended, log_sum.T),
        1 << 18,
        name="pack",
    )
    qds = [qd] + [x_from(qd, k) for k in (1, 2, 3)]
    qd_far = swap(jnp.stack(qds))

    owner = chosen >> 3
    inner = chosen & 7
    listed = chosen >= 0
    peer = jnp.where(c == 0, (owner & 7) * 8 + (owner >> 3), owner)
    slot = jnp.where(listed, jnp.where(owner == rank, PEERS + inner, peer), 0)
    starts = rank * TOK + lax.broadcasted_iota(jnp.int32, chosen.shape, 0) * BLOCK
    rel = jnp.where(listed, chosen * BLOCK + ROWS * tp - starts, FAR)

    away, own, gq_own, gq_far = call(
        attend_kernel,
        [SMEM] * 2 + [VMEM] * 7,
        [
            held((PEERS, ROWS, LANES), BF16),
            held((BLOCKS, ROWS, LANES), F32),
            held((4, TOK, LANES), F32),
            held((4, TOK, LANES), BF16),
        ],
        (slot, rel, near_core(fetched), near_core(piece), *map(near_core, qds), near_core(qd_far)),
        1 << 30,
        scratch_shapes=[
            pltpu.VMEM((BLOCKS, 8, TOK), F32),
            pltpu.VMEM((PEERS + BLOCKS, ROWS, LANES), F32),
            pltpu.VMEM((PEERS + BLOCKS, ROWS, LANES), F32),
        ],
        name="attend",
    )
    gq4 = gq_own + swap(gq_far).astype(F32)
    given = along(away.reshape(SIDE, SIDE, ROWS, LANES), False)
    relayed = call(
        relay_kernel,
        [VMEM] * 2,
        held((SIDE, BLOCKS, ROWS, LANES), BF16),
        (near_core(wants), near_core(given)),
        1 << 20,
        name="relay",
    )
    returned = along(relayed, True)
    gq = gq4[0]
    for k in (1, 2, 3):
        gq = gq + x_back(gq4[k].astype(BF16), k).astype(F32)
    grad_queries = gq.astype(BF16)
    part = lax.dot_general(
        normed, grad_queries, (((0,), (0,)), ((), ())), preferred_element_type=F32
    ).astype(BF16)
    parts = exchange(part.reshape(PEERS, BLOCK, LANES))
    weight_grad = jnp.sum(parts.astype(F32), axis=0)

    total = call(
        settle_kernel,
        [VMEM] * 2,
        held((BLOCKS, ROWS, LANES), F32),
        (near_core(own), near_core(returned)),
        1 << 20,
        name="settle",
    )
    near = jnp.stack([total] + [x_from(total, k) for k in (1, 2, 3)])
    far = swap(near)
    grad_keys, grad_values = call(
        place_kernel,
        [SMEM, VMEM, VMEM],
        [sds((64, TOK), F32), sds((64, TOK), F32)],
        (tp.reshape(1), near_core(near), near_core(far)),
        1 << 20,
        scratch_shapes=[pltpu.VMEM((TOK, LANES), F32)],
        name="place",
    )
    return grad_queries, grad_keys.T, grad_values.T, weight_grad


def solution(mesh):
    torus = Mesh(mesh.devices.reshape(8, 8, 4, 2), ("z", "y", "x", "c"))
    heads = ("x", "c")
    in_specs = (
        P(KV, None),
        P(KV, heads),
        P(KV, None),
        P(KV, None),
        P(KV, heads),
        P(KV, heads),
        P(KV, heads),
        P(KV, None),
    )
    out_specs = (P(KV, heads), P(KV, None), P(KV, None), P(KV, heads))
    return jax.shard_map(step, mesh=torus, in_specs=in_specs, out_specs=out_specs, check_vma=False)
```

```python
import jax
import jax.numpy as jnp
from jax import lax
from jax.experimental import pallas as pl
from jax.experimental.pallas import tpu as pltpu
from jax.sharding import Mesh
from jax.sharding import PartitionSpec as P


BLOCK = 64
BLOCKS = 8
SLOTS = 16
PEERS = 64
SIDE = 8
ROWS = 8
TOK = 512
LANES = 128
SCALE = 0.125
KV = ("z", "y")
ALL = ("z", "y", "x", "c")
FAR = 1 << 20
F32 = jnp.float32
BF16 = jnp.bfloat16
VMEM = pl.BlockSpec(memory_space=pltpu.VMEM)
SMEM = pl.BlockSpec(memory_space=pltpu.SMEM)


def low_lanes(shape):
    return lax.broadcasted_iota(jnp.int32, shape, len(shape) - 1) < LANES // 2


def offer_kernel(rank_ref, tp_ref, keys_ref, vals_ref, chosen_ref, out_ref, piece_ref, want_ref, pairs):
    rank = rank_ref[0]
    tp = tp_ref[0]
    flip = tp & 1
    both = jnp.concatenate([keys_ref[...], vals_ref[...]], axis=0).astype(F32)
    pairs[...] = both.T
    at = lax.broadcasted_iota(jnp.int32, (PEERS, SLOTS), 0)

    def wanted(peer):
        best = jnp.zeros((PEERS, SLOTS), jnp.int32)
        for j in range(BLOCKS):
            c = chosen_ref[j : j + 1, :]
            hit = ((c >> 3) == peer) & (c >= 0) & (peer != rank)
            best = jnp.maximum(best, jnp.where(hit, (c & 7) + 1, 0))
        best = jnp.max(best, axis=1, keepdims=True)
        return jnp.broadcast_to(best, (PEERS, LANES)).astype(F32)

    best = wanted(jnp.where(jnp.full(at.shape, flip, jnp.int32) == 0, at, (at & 7) * 8 + (at >> 3)))
    want_ref[...] = wanted(at)
    for b in range(BLOCKS):
        at = pl.multiple_of(b * BLOCK + tp * ROWS, ROWS)
        piece = pairs[pl.ds(at, ROWS), :].astype(BF16)
        piece_ref[b] = piece
        for i in range(SIDE):
            out_ref[i, b] = piece
    for i in range(SIDE):
        out_ref[i, BLOCKS] = best[i * SIDE : (i + 1) * SIDE].astype(BF16)


def pick_kernel(wants_ref, pushed_ref, out_ref):
    for r in range(SIDE):
        pieces = [pushed_ref[r, b].astype(F32) for b in range(BLOCKS)]
        for i in range(SIDE):
            want = jnp.broadcast_to(wants_ref[i].astype(F32)[r : r + 1], (ROWS, LANES))
            got = jnp.zeros((ROWS, LANES), F32)
            for b in range(BLOCKS):
                got = jnp.where(want == b + 1.0, pieces[b], got)
            out_ref[i, r] = got.astype(BF16)


def settle_kernel(own_ref, given_ref, out_ref):
    totals = [own_ref[b] for b in range(BLOCKS)]
    for s in range(PEERS):
        got = given_ref[s, :ROWS].astype(F32)
        want = given_ref[s, ROWS:].astype(F32)
        for b in range(BLOCKS):
            totals[b] = totals[b] + jnp.where(want == b + 1.0, got, 0.0)
    for b in range(BLOCKS):
        out_ref[b] = totals[b]


def pack_kernel(q_ref, g_ref, o_ref, log_ref, out_ref):
    out_ref[0:TOK] = q_ref[...]
    out_ref[TOK : 2 * TOK] = g_ref[...]
    prod = (g_ref[...].astype(F32) * o_ref[...].astype(F32)).T
    half = LANES // 2
    stats = jnp.concatenate(
        [
            log_ref[...],
            jnp.sum(prod[:half], axis=0, keepdims=True),
            jnp.sum(prod[half:], axis=0, keepdims=True),
        ],
        axis=0,
    )
    rest = jnp.concatenate([stats[:, m * LANES : (m + 1) * LANES] for m in range(4)], axis=0)
    for n in range(3):
        part = rest.astype(BF16)
        out_ref[2 * TOK + 16 * n : 2 * TOK + 16 * (n + 1)] = part
        rest = rest - part.astype(F32)


def attend_kernel(
    slot_ref,
    home_ref,
    rel_ref,
    fetched_ref,
    piece_ref,
    want_ref,
    q0,
    q1,
    q2,
    q3,
    qp_ref,
    away_ref,
    own_ref,
    gq_own_ref,
    gq_far_ref,
    stats_tab,
    table,
    acc,
):
    near = (q0, q1, q2, q3)
    table[:PEERS] = fetched_ref[...].astype(F32)
    table[PEERS:] = piece_ref[...].astype(F32)
    acc[...] = jnp.zeros(acc.shape, F32)
    low = low_lanes((LANES, LANES))
    low4 = low_lanes((4, LANES))
    row8 = lax.broadcasted_iota(jnp.int32, (ROWS, LANES), 0)
    query_t = lax.broadcasted_iota(jnp.int32, (LANES, LANES), 1) & (BLOCK - 1)

    def stat(p):
        parts = []
        for n in range(3):
            at = 2 * TOK + 16 * n
            parts.append((near[p][at : at + 16, :] if p < 4 else qp_ref[p - 4, at : at + 16, :]).astype(F32))
        return parts[0] + parts[1] + parts[2]

    for pair in range(4):
        even, odd = stat(2 * pair), stat(2 * pair + 1)
        even_turned = pltpu.roll(even, LANES // 2, 1)
        odd_turned = pltpu.roll(odd, LANES // 2, 1)
        for j in range(BLOCKS):
            m = 4 * (j // 2)
            lo = even[m : m + 4] if j % 2 == 0 else even_turned[m : m + 4]
            hi = odd_turned[m : m + 4] if j % 2 == 0 else odd[m : m + 4]
            stats_tab[j, 0:4, pair * LANES : (pair + 1) * LANES] = jnp.where(low4, lo, hi)

    def one_block(j, carry):
        kv = jnp.concatenate([table[slot_ref[j, s]] for s in range(SLOTS)], axis=0)
        turned = pltpu.roll(kv, LANES // 2, 1)
        k2 = jnp.concatenate([jnp.where(low, kv, 0.0), jnp.where(low, 0.0, turned)], axis=0).astype(BF16)
        v2 = jnp.concatenate([jnp.where(low, turned, 0.0), jnp.where(low, 0.0, kv)], axis=0).astype(BF16)
        at = pl.multiple_of(j * BLOCK, BLOCK)
        q = jnp.concatenate(
            [r[pl.ds(at, BLOCK), :] for r in near]
            + [qp_ref[k, pl.ds(at, BLOCK), :] for k in range(4)],
            axis=0,
        )
        g = jnp.concatenate(
            [r[pl.ds(TOK + at, BLOCK), :] for r in near]
            + [qp_ref[k, pl.ds(TOK + at, BLOCK), :] for k in range(4)],
            axis=0,
        )
        last = (((1,), (1,)), ((), ()))
        scores = lax.dot_general(k2, q, last, preferred_element_type=F32)
        dprobs = lax.dot_general(v2, g, last, preferred_element_type=F32)
        rel = jnp.concatenate([row8 + rel_ref[j, s] for s in range(SLOTS)], axis=0)
        seen = (rel <= query_t).astype(F32)
        seen = jnp.concatenate([seen] * 4, axis=1) > 0.0
        stat_j = stats_tab[j]
        probs = []
        dscores = []
        for h in range(2):
            s = scores[h * LANES : (h + 1) * LANES]
            d = dprobs[h * LANES : (h + 1) * LANES]
            p = jnp.where(seen, jnp.exp(s * SCALE - stat_j[h : h + 1, :]), 0.0)
            probs.append(p.astype(BF16))
            dscores.append((p * (d - stat_j[2 + h : 3 + h, :]) * SCALE).astype(BF16))
        probs = jnp.concatenate(probs, axis=0)
        dscores = jnp.concatenate(dscores, axis=0)
        plain = (((1,), (0,)), ((), ()))
        dv = lax.dot_general(probs, g, plain, preferred_element_type=F32)
        dk = lax.dot_general(dscores, q, plain, preferred_element_type=F32)
        gq = lax.dot_general(dscores, k2, (((0,), (0,)), ((), ())), preferred_element_type=F32)
        for k in range(4):
            gq_own_ref[k, pl.ds(at, BLOCK), :] = gq[k * BLOCK : (k + 1) * BLOCK]
            gq_far_ref[k, pl.ds(at, BLOCK), :] = gq[(4 + k) * BLOCK : (5 + k) * BLOCK].astype(BF16)
        both = jnp.where(low, dk[:LANES], dv[LANES:]) + pltpu.roll(
            jnp.where(low, dv[:LANES], dk[LANES:]), LANES // 2, 1
        )
        for s in range(SLOTS):
            acc[home_ref[j, s]] += both[s * ROWS : (s + 1) * ROWS]
        return carry

    lax.fori_loop(0, BLOCKS, one_block, 0)
    away_ref[:, :ROWS] = acc[:PEERS].astype(BF16)
    for s in range(PEERS):
        want = jnp.broadcast_to(want_ref[s : s + 1, :], (ROWS, LANES))
        away_ref[s, ROWS:] = want.astype(BF16)
    own_ref[...] = acc[PEERS:]


def place_kernel(tp_ref, near_ref, far_ref, keys_ref, vals_ref, rows):
    x = tp_ref[0] >> 1
    mine = jnp.full((ROWS, LANES), tp_ref[0] & 1, jnp.int32)
    for xa in range(4):
        k = (x + 4 - xa) & 3
        for ca in range(2):
            for b in range(BLOCKS):
                at = b * BLOCK + (xa * 2 + ca) * ROWS
                rows[at : at + ROWS, :] = jnp.where(mine == ca, near_ref[k, b], far_ref[k, b])
    turned = rows[...].T
    keys_ref[...] = turned[: LANES // 2]
    vals_ref[...] = turned[LANES // 2 :]


def call(kernel, ins, out_shape, args, flops, limit=8 << 20, **kw):
    many = isinstance(out_shape, (list, tuple))
    return pl.pallas_call(
        kernel,
        in_specs=ins,
        out_specs=[VMEM] * len(out_shape) if many else VMEM,
        out_shape=out_shape,
        cost_estimate=pl.CostEstimate(flops=flops, bytes_accessed=1 << 20, transcendentals=0),
        compiler_params=pltpu.CompilerParams(vmem_limit_bytes=limit),
        **kw,
    )(*args)


def sds(shape, dtype):
    return jax.ShapeDtypeStruct(shape, dtype)


def held(shape, dtype):
    return pltpu.VMEM(shape, dtype)


def x_from(arr, k):
    return lax.ppermute(arr, "x", [(i, (i + k) % 4) for i in range(4)])


def x_back(arr, k):
    return lax.ppermute(arr, "x", [((i + k) % 4, i) for i in range(4)])


def swap(arr):
    return lax.ppermute(arr, "c", [(0, 1), (1, 0)])


def device(z, y, x, c):
    return ((z * 8 + y) * 4 + x) * 2 + c


def lines(first):
    out = []
    for x in range(4):
        for c in range(2):
            for a in range(SIDE):
                if (c == 0) == first:
                    out.append([device(i, a, x, c) for i in range(SIDE)])
                else:
                    out.append([device(a, i, x, c) for i in range(SIDE)])
    return out


def along(arr, first):
    return lax.all_to_all(
        arr, ALL, split_axis=0, concat_axis=0, tiled=True, axis_index_groups=lines(first)
    )


def exchange(arr):
    return lax.all_to_all(arr, KV, split_axis=0, concat_axis=0, tiled=True)


def near_core(arr):
    return pltpu.with_memory_space_constraint(arr, pltpu.VMEM)


def step(normed, queries, keys, values, attended, cotangent, log_sum, chosen):
    rank = lax.axis_index(KV).astype(jnp.int32)
    x = lax.axis_index("x").astype(jnp.int32)
    c = lax.axis_index("c").astype(jnp.int32)
    tp = x * 2 + c
    offer, piece, want = call(
        offer_kernel,
        [SMEM] * 2 + [VMEM] * 3,
        [
            sds((SIDE, BLOCKS + 1, ROWS, LANES), BF16),
            sds((BLOCKS, ROWS, LANES), BF16),
            sds((PEERS, LANES), F32),
        ],
        (rank.reshape(1), tp.reshape(1), keys.T, values.T, chosen),
        1 << 18,
        limit=58 << 20,
        scratch_shapes=[pltpu.VMEM((TOK, LANES), F32)],
        name="offer",
    )
    pushed = along(offer, True)
    wants = swap(pushed[:, BLOCKS])
    picked = call(
        pick_kernel,
        [VMEM] * 2,
        held((SIDE, SIDE, ROWS, LANES), BF16),
        (near_core(wants), near_core(pushed)),
        1 << 20,
        name="pick",
    )
    fetched = along(picked, False).reshape(PEERS, ROWS, LANES)

    qd = call(
        pack_kernel,
        [VMEM] * 4,
        sds((2 * TOK + 48, LANES), BF16),
        (queries, cotangent, attended, log_sum.T),
        1 << 18,
        limit=58 << 20,
        name="pack",
    )
    qds = [qd] + [x_from(qd, k) for k in (1, 2, 3)]
    qd_far = swap(jnp.stack(qds))

    owner = chosen >> 3
    inner = chosen & 7
    listed = chosen >= 0
    peer = jnp.where(c == 0, (owner & 7) * 8 + (owner >> 3), owner)
    slot = jnp.where(listed, jnp.where(owner == rank, PEERS + inner, peer), 0)
    starts = rank * TOK + lax.broadcasted_iota(jnp.int32, chosen.shape, 0) * BLOCK
    home = jnp.where(listed, jnp.where(owner == rank, PEERS + inner, owner), 0)
    rel = jnp.where(listed, chosen * BLOCK + ROWS * tp - starts, FAR)

    away, own, gq_own, gq_far = call(
        attend_kernel,
        [SMEM] * 3 + [VMEM] * 8,
        [
            held((PEERS, 2 * ROWS, LANES), BF16),
            held((BLOCKS, ROWS, LANES), F32),
            held((4, TOK, LANES), F32),
            held((4, TOK, LANES), BF16),
        ],
        (slot, home, rel, near_core(fetched), near_core(piece), near_core(want), *map(near_core, qds), near_core(qd_far)),
        1 << 30,
        limit=16 << 20,
        scratch_shapes=[
            pltpu.VMEM((BLOCKS, 8, TOK), F32),
            pltpu.VMEM((PEERS + BLOCKS, ROWS, LANES), F32),
            pltpu.VMEM((PEERS + BLOCKS, ROWS, LANES), F32),
        ],
        name="attend",
    )
    gq4 = gq_own + swap(gq_far).astype(F32)
    returned = exchange(away)
    gq = gq4[0]
    for k in (1, 2, 3):
        gq = gq + x_back(gq4[k].astype(BF16), k).astype(F32)
    grad_queries = gq.astype(BF16)
    part = lax.dot_general(
        normed, grad_queries, (((0,), (0,)), ((), ())), preferred_element_type=F32
    ).astype(BF16)
    parts = exchange(part.reshape(PEERS, BLOCK, LANES))
    weight_grad = jnp.sum(parts.astype(F32), axis=0)

    total = call(
        settle_kernel,
        [VMEM] * 2,
        held((BLOCKS, ROWS, LANES), F32),
        (near_core(own), near_core(returned)),
        1 << 20,
        name="settle",
    )
    near = jnp.stack([total] + [x_from(total, k) for k in (1, 2, 3)])
    far = swap(near)
    grad_keys, grad_values = call(
        place_kernel,
        [SMEM, VMEM, VMEM],
        [sds((64, TOK), F32), sds((64, TOK), F32)],
        (tp.reshape(1), near_core(near), near_core(far)),
        1 << 20,
        scratch_shapes=[pltpu.VMEM((TOK, LANES), F32)],
        name="place",
    )
    return grad_queries, grad_keys.T, grad_values.T, weight_grad


def solution(mesh):
    torus = Mesh(mesh.devices.reshape(8, 8, 4, 2), ("z", "y", "x", "c"))
    heads = ("x", "c")
    in_specs = (
        P(KV, None),
        P(KV, heads),
        P(KV, None),
        P(KV, None),
        P(KV, heads),
        P(KV, heads),
        P(KV, heads),
        P(KV, None),
    )
    out_specs = (P(KV, heads), P(KV, None), P(KV, None), P(KV, heads))
    return jax.shard_map(step, mesh=torus, in_specs=in_specs, out_specs=out_specs, check_vma=False)
```

```python
import jax
import jax.numpy as jnp
from jax import lax
from jax.experimental import pallas as pl
from jax.experimental.pallas import tpu as pltpu
from jax.sharding import Mesh
from jax.sharding import PartitionSpec as P


BLOCK = 64
BLOCKS = 8
SLOTS = 16
PEERS = 64
SIDE = 8
ROWS = 8
TOK = 512
LANES = 128
SCALE = 0.125
KV = ("z", "y")
TP = ("x", "c")
ALL = ("z", "y", "x", "c")
FAR = 1 << 20
F32 = jnp.float32
BF16 = jnp.bfloat16
VMEM = pl.BlockSpec(memory_space=pltpu.VMEM)
SMEM = pl.BlockSpec(memory_space=pltpu.SMEM)


def low_lanes(shape):
    return lax.broadcasted_iota(jnp.int32, shape, len(shape) - 1) < LANES // 2


def offer_kernel(rank_ref, tp_ref, keys_ref, vals_ref, chosen_ref, out_ref, piece_ref, want_ref, pairs):
    rank = rank_ref[0]
    tp = tp_ref[0]
    flip = tp & 1
    both = jnp.concatenate([keys_ref[...], vals_ref[...]], axis=0).astype(F32)
    pairs[...] = both.T
    at = lax.broadcasted_iota(jnp.int32, (PEERS, SLOTS), 0)

    def wanted(peer):
        best = jnp.zeros((PEERS, SLOTS), jnp.int32)
        for j in range(BLOCKS):
            c = chosen_ref[j : j + 1, :]
            hit = ((c >> 3) == peer) & (c >= 0) & (peer != rank)
            best = jnp.maximum(best, jnp.where(hit, (c & 7) + 1, 0))
        best = jnp.max(best, axis=1, keepdims=True)
        return jnp.broadcast_to(best, (PEERS, LANES)).astype(F32)

    best = wanted(jnp.where(jnp.full(at.shape, flip, jnp.int32) == 0, at, (at & 7) * 8 + (at >> 3)))
    want_ref[...] = wanted(at)
    for b in range(BLOCKS):
        at = pl.multiple_of(b * BLOCK + tp * ROWS, ROWS)
        piece = pairs[pl.ds(at, ROWS), :].astype(BF16)
        piece_ref[b] = piece
        for i in range(SIDE):
            out_ref[i, b] = piece
    for i in range(SIDE):
        out_ref[i, BLOCKS] = best[i * SIDE : (i + 1) * SIDE].astype(BF16)


def pick_kernel(wants_ref, pushed_ref, out_ref):
    for r in range(SIDE):
        pieces = [pushed_ref[r, b].astype(F32) for b in range(BLOCKS)]
        for i in range(SIDE):
            want = jnp.broadcast_to(wants_ref[i].astype(F32)[r : r + 1], (ROWS, LANES))
            got = jnp.zeros((ROWS, LANES), F32)
            for b in range(BLOCKS):
                got = jnp.where(want == b + 1.0, pieces[b], got)
            out_ref[i, r] = got.astype(BF16)


def settle_kernel(own_ref, given_ref, out_ref):
    totals = [own_ref[b] for b in range(BLOCKS)]
    for s in range(PEERS):
        got = given_ref[s, :ROWS].astype(F32)
        want = given_ref[s, ROWS:].astype(F32)
        for b in range(BLOCKS):
            totals[b] = totals[b] + jnp.where(want == b + 1.0, got, 0.0)
    for i in range(SIDE):
        for b in range(BLOCKS):
            out_ref[i, b] = totals[b]


def pack_kernel(q_ref, g_ref, o_ref, log_ref, out_ref):
    out_ref[0:TOK] = q_ref[...]
    out_ref[TOK : 2 * TOK] = g_ref[...]
    prod = (g_ref[...].astype(F32) * o_ref[...].astype(F32)).T
    half = LANES // 2
    stats = jnp.concatenate(
        [
            log_ref[...],
            jnp.sum(prod[:half], axis=0, keepdims=True),
            jnp.sum(prod[half:], axis=0, keepdims=True),
        ],
        axis=0,
    )
    rest = jnp.concatenate([stats[:, m * LANES : (m + 1) * LANES] for m in range(4)], axis=0)
    for n in range(3):
        part = rest.astype(BF16)
        out_ref[2 * TOK + 16 * n : 2 * TOK + 16 * (n + 1)] = part
        rest = rest - part.astype(F32)


def attend_kernel(
    slot_ref,
    home_ref,
    rel_ref,
    fetched_ref,
    piece_ref,
    want_ref,
    q0,
    q1,
    q2,
    q3,
    qp_ref,
    away_ref,
    own_ref,
    gq_own_ref,
    gq_far_ref,
    stats_tab,
    table,
    acc,
):
    near = (q0, q1, q2, q3)
    table[:PEERS] = fetched_ref[...].astype(F32)
    table[PEERS:] = piece_ref[...].astype(F32)
    acc[...] = jnp.zeros(acc.shape, F32)
    low = low_lanes((LANES, LANES))
    low4 = low_lanes((4, LANES))
    row8 = lax.broadcasted_iota(jnp.int32, (ROWS, LANES), 0)
    query_t = lax.broadcasted_iota(jnp.int32, (LANES, LANES), 1) & (BLOCK - 1)

    def stat(p):
        parts = []
        for n in range(3):
            at = 2 * TOK + 16 * n
            parts.append((near[p][at : at + 16, :] if p < 4 else qp_ref[p - 4, at : at + 16, :]).astype(F32))
        return parts[0] + parts[1] + parts[2]

    for pair in range(4):
        even, odd = stat(2 * pair), stat(2 * pair + 1)
        even_turned = pltpu.roll(even, LANES // 2, 1)
        odd_turned = pltpu.roll(odd, LANES // 2, 1)
        for j in range(BLOCKS):
            m = 4 * (j // 2)
            lo = even[m : m + 4] if j % 2 == 0 else even_turned[m : m + 4]
            hi = odd_turned[m : m + 4] if j % 2 == 0 else odd[m : m + 4]
            stats_tab[j, 0:4, pair * LANES : (pair + 1) * LANES] = jnp.where(low4, lo, hi)

    def one_block(j, carry):
        kv = jnp.concatenate([table[slot_ref[j, s]] for s in range(SLOTS)], axis=0)
        turned = pltpu.roll(kv, LANES // 2, 1)
        k2 = jnp.concatenate([jnp.where(low, kv, 0.0), jnp.where(low, 0.0, turned)], axis=0).astype(BF16)
        v2 = jnp.concatenate([jnp.where(low, turned, 0.0), jnp.where(low, 0.0, kv)], axis=0).astype(BF16)
        at = pl.multiple_of(j * BLOCK, BLOCK)
        q = jnp.concatenate(
            [r[pl.ds(at, BLOCK), :] for r in near]
            + [qp_ref[k, pl.ds(at, BLOCK), :] for k in range(4)],
            axis=0,
        )
        g = jnp.concatenate(
            [r[pl.ds(TOK + at, BLOCK), :] for r in near]
            + [qp_ref[k, pl.ds(TOK + at, BLOCK), :] for k in range(4)],
            axis=0,
        )
        last = (((1,), (1,)), ((), ()))
        scores = lax.dot_general(k2, q, last, preferred_element_type=F32)
        dprobs = lax.dot_general(v2, g, last, preferred_element_type=F32)
        rel = jnp.concatenate([row8 + rel_ref[j, s] for s in range(SLOTS)], axis=0)
        seen = (rel <= query_t).astype(F32)
        seen = jnp.concatenate([seen] * 4, axis=1) > 0.0
        stat_j = stats_tab[j]
        probs = []
        dscores = []
        for h in range(2):
            s = scores[h * LANES : (h + 1) * LANES]
            d = dprobs[h * LANES : (h + 1) * LANES]
            p = jnp.where(seen, jnp.exp(s * SCALE - stat_j[h : h + 1, :]), 0.0)
            probs.append(p.astype(BF16))
            dscores.append((p * (d - stat_j[2 + h : 3 + h, :]) * SCALE).astype(BF16))
        probs = jnp.concatenate(probs, axis=0)
        dscores = jnp.concatenate(dscores, axis=0)
        plain = (((1,), (0,)), ((), ()))
        dv = lax.dot_general(probs, g, plain, preferred_element_type=F32)
        dk = lax.dot_general(dscores, q, plain, preferred_element_type=F32)
        gq = lax.dot_general(dscores, k2, (((0,), (0,)), ((), ())), preferred_element_type=F32)
        for k in range(4):
            gq_own_ref[k, pl.ds(at, BLOCK), :] = gq[k * BLOCK : (k + 1) * BLOCK]
            gq_far_ref[k, pl.ds(at, BLOCK), :] = gq[(4 + k) * BLOCK : (5 + k) * BLOCK].astype(BF16)
        both = jnp.where(low, dk[:LANES], dv[LANES:]) + pltpu.roll(
            jnp.where(low, dv[:LANES], dk[LANES:]), LANES // 2, 1
        )
        for s in range(SLOTS):
            acc[home_ref[j, s]] += both[s * ROWS : (s + 1) * ROWS]
        return carry

    lax.fori_loop(0, BLOCKS, one_block, 0)
    away_ref[:, :ROWS] = acc[:PEERS].astype(BF16)
    for s in range(PEERS):
        want = jnp.broadcast_to(want_ref[s : s + 1, :], (ROWS, LANES))
        away_ref[s, ROWS:] = want.astype(BF16)
    own_ref[...] = acc[PEERS:]


def place_kernel(pieces_ref, keys_ref, vals_ref, rows):
    for i in range(SIDE):
        for b in range(BLOCKS):
            at = b * BLOCK + i * ROWS
            rows[at : at + ROWS, :] = pieces_ref[i, b]
    turned = rows[...].T
    keys_ref[...] = turned[: LANES // 2]
    vals_ref[...] = turned[LANES // 2 :]


def call(kernel, ins, out_shape, args, flops, limit=8 << 20, **kw):
    many = isinstance(out_shape, (list, tuple))
    return pl.pallas_call(
        kernel,
        in_specs=ins,
        out_specs=[VMEM] * len(out_shape) if many else VMEM,
        out_shape=out_shape,
        cost_estimate=pl.CostEstimate(flops=flops, bytes_accessed=1 << 20, transcendentals=0),
        compiler_params=pltpu.CompilerParams(vmem_limit_bytes=limit),
        **kw,
    )(*args)


def sds(shape, dtype):
    return jax.ShapeDtypeStruct(shape, dtype)


def held(shape, dtype):
    return pltpu.VMEM(shape, dtype)


def x_from(arr, k):
    return lax.ppermute(arr, "x", [(i, (i + k) % 4) for i in range(4)])


def x_back(arr, k):
    return lax.ppermute(arr, "x", [((i + k) % 4, i) for i in range(4)])


def swap(arr):
    return lax.ppermute(arr, "c", [(0, 1), (1, 0)])


def device(z, y, x, c):
    return ((z * 8 + y) * 4 + x) * 2 + c


def lines(first):
    out = []
    for x in range(4):
        for c in range(2):
            for a in range(SIDE):
                if (c == 0) == first:
                    out.append([device(i, a, x, c) for i in range(SIDE)])
                else:
                    out.append([device(a, i, x, c) for i in range(SIDE)])
    return out


def along(arr, first):
    return lax.all_to_all(
        arr, ALL, split_axis=0, concat_axis=0, tiled=True, axis_index_groups=lines(first)
    )


def exchange(arr):
    return lax.all_to_all(arr, KV, split_axis=0, concat_axis=0, tiled=True)


def near_core(arr):
    return pltpu.with_memory_space_constraint(arr, pltpu.VMEM)


def step(normed, queries, keys, values, attended, cotangent, log_sum, chosen):
    rank = lax.axis_index(KV).astype(jnp.int32)
    x = lax.axis_index("x").astype(jnp.int32)
    c = lax.axis_index("c").astype(jnp.int32)
    tp = x * 2 + c
    offer, piece, want = call(
        offer_kernel,
        [SMEM] * 2 + [VMEM] * 3,
        [
            sds((SIDE, BLOCKS + 1, ROWS, LANES), BF16),
            sds((BLOCKS, ROWS, LANES), BF16),
            sds((PEERS, LANES), F32),
        ],
        (rank.reshape(1), tp.reshape(1), keys.T, values.T, chosen),
        1 << 18,
        limit=58 << 20,
        scratch_shapes=[pltpu.VMEM((TOK, LANES), F32)],
        name="offer",
    )
    pushed = along(offer, True)
    wants = swap(pushed[:, BLOCKS])
    picked = call(
        pick_kernel,
        [VMEM] * 2,
        held((SIDE, SIDE, ROWS, LANES), BF16),
        (near_core(wants), near_core(pushed)),
        1 << 20,
        name="pick",
    )
    fetched = along(picked, False).reshape(PEERS, ROWS, LANES)

    qd = call(
        pack_kernel,
        [VMEM] * 4,
        sds((2 * TOK + 48, LANES), BF16),
        (queries, cotangent, attended, log_sum.T),
        1 << 18,
        limit=58 << 20,
        name="pack",
    )
    qds = [qd] + [x_from(qd, k) for k in (1, 2, 3)]
    qd_far = swap(jnp.stack(qds))

    owner = chosen >> 3
    inner = chosen & 7
    listed = chosen >= 0
    peer = jnp.where(c == 0, (owner & 7) * 8 + (owner >> 3), owner)
    slot = jnp.where(listed, jnp.where(owner == rank, PEERS + inner, peer), 0)
    starts = rank * TOK + lax.broadcasted_iota(jnp.int32, chosen.shape, 0) * BLOCK
    home = jnp.where(listed, jnp.where(owner == rank, PEERS + inner, owner), 0)
    rel = jnp.where(listed, chosen * BLOCK + ROWS * tp - starts, FAR)

    away, own, gq_own, gq_far = call(
        attend_kernel,
        [SMEM] * 3 + [VMEM] * 8,
        [
            held((PEERS, 2 * ROWS, LANES), BF16),
            held((BLOCKS, ROWS, LANES), F32),
            held((4, TOK, LANES), F32),
            held((4, TOK, LANES), BF16),
        ],
        (slot, home, rel, near_core(fetched), near_core(piece), near_core(want), *map(near_core, qds), near_core(qd_far)),
        1 << 30,
        limit=16 << 20,
        scratch_shapes=[
            pltpu.VMEM((BLOCKS, 8, TOK), F32),
            pltpu.VMEM((PEERS + BLOCKS, ROWS, LANES), F32),
            pltpu.VMEM((PEERS + BLOCKS, ROWS, LANES), F32),
        ],
        name="attend",
    )
    gq4 = gq_own + swap(gq_far).astype(F32)
    returned = exchange(away)
    gq = gq4[0]
    for k in (1, 2, 3):
        gq = gq + x_back(gq4[k].astype(BF16), k).astype(F32)
    grad_queries = gq.astype(BF16)
    part = lax.dot_general(
        normed, grad_queries, (((0,), (0,)), ((), ())), preferred_element_type=F32
    ).astype(BF16)
    parts = exchange(part.reshape(PEERS, BLOCK, LANES))
    weight_grad = jnp.sum(parts.astype(F32), axis=0)

    total = call(
        settle_kernel,
        [VMEM] * 2,
        held((SIDE, BLOCKS, ROWS, LANES), F32),
        (near_core(own), near_core(returned)),
        1 << 20,
        name="settle",
    )
    pieces = lax.all_to_all(total, TP, split_axis=0, concat_axis=0, tiled=True)
    grad_keys, grad_values = call(
        place_kernel,
        [VMEM],
        [sds((64, TOK), F32), sds((64, TOK), F32)],
        (near_core(pieces),),
        1 << 20,
        scratch_shapes=[pltpu.VMEM((TOK, LANES), F32)],
        name="place",
    )
    return grad_queries, grad_keys.T, grad_values.T, weight_grad


def solution(mesh):
    torus = Mesh(mesh.devices.reshape(8, 8, 4, 2), ("z", "y", "x", "c"))
    heads = ("x", "c")
    in_specs = (
        P(KV, None),
        P(KV, heads),
        P(KV, None),
        P(KV, None),
        P(KV, heads),
        P(KV, heads),
        P(KV, heads),
        P(KV, None),
    )
    out_specs = (P(KV, heads), P(KV, None), P(KV, None), P(KV, heads))
    return jax.shard_map(step, mesh=torus, in_specs=in_specs, out_specs=out_specs, check_vma=False)
```

```python
import jax
import jax.numpy as jnp
from jax import lax
from jax.experimental import pallas as pl
from jax.experimental.pallas import tpu as pltpu
from jax.sharding import Mesh
from jax.sharding import PartitionSpec as P


BLOCK = 64
BLOCKS = 8
SLOTS = 16
PEERS = 64
SIDE = 8
ROWS = 8
TOK = 512
LANES = 128
SCALE = 0.125
LOG2E = 1.4426950408889634
KV = ("z", "y")
ALL = ("z", "y", "x", "c")
FAR = 1 << 20
F32 = jnp.float32
BF16 = jnp.bfloat16
VMEM = pl.BlockSpec(memory_space=pltpu.VMEM)
SMEM = pl.BlockSpec(memory_space=pltpu.SMEM)


def low_lanes(shape):
    return lax.broadcasted_iota(jnp.int32, shape, len(shape) - 1) < LANES // 2


def offer_kernel(rank_ref, tp_ref, keys_ref, vals_ref, chosen_ref, out_ref, piece_ref, want_ref, pairs):
    rank = rank_ref[0]
    tp = tp_ref[0]
    flip = tp & 1
    both = jnp.concatenate([keys_ref[...], vals_ref[...]], axis=0).astype(F32)
    pairs[...] = both.T
    at = lax.broadcasted_iota(jnp.int32, (PEERS, SLOTS), 0)

    def wanted(peer):
        best = jnp.zeros((PEERS, SLOTS), jnp.int32)
        for j in range(BLOCKS):
            c = chosen_ref[j : j + 1, :]
            hit = ((c >> 3) == peer) & (c >= 0) & (peer != rank)
            best = jnp.maximum(best, jnp.where(hit, (c & 7) + 1, 0))
        best = jnp.max(best, axis=1, keepdims=True)
        return jnp.broadcast_to(best, (PEERS, LANES)).astype(F32)

    best = wanted(jnp.where(jnp.full(at.shape, flip, jnp.int32) == 0, at, (at & 7) * 8 + (at >> 3)))
    want_ref[...] = wanted(at)
    for b in range(BLOCKS):
        at = pl.multiple_of(b * BLOCK + tp * ROWS, ROWS)
        piece = pairs[pl.ds(at, ROWS), :].astype(BF16)
        piece_ref[b] = piece
        for i in range(SIDE):
            out_ref[i, b] = piece
    for i in range(SIDE):
        out_ref[i, BLOCKS] = best[i * SIDE : (i + 1) * SIDE].astype(BF16)


def pick_kernel(wants_ref, pushed_ref, out_ref):
    for r in range(SIDE):
        pieces = [pushed_ref[r, b].astype(F32) for b in range(BLOCKS)]
        for i in range(SIDE):
            want = jnp.broadcast_to(wants_ref[i].astype(F32)[r : r + 1], (ROWS, LANES))
            got = jnp.zeros((ROWS, LANES), F32)
            for b in range(BLOCKS):
                got = jnp.where(want == b + 1.0, pieces[b], got)
            out_ref[i, r] = got.astype(BF16)


def settle_kernel(own_ref, given_ref, out_ref):
    totals = [own_ref[b] for b in range(BLOCKS)]
    for s in range(PEERS):
        got = given_ref[s, :ROWS].astype(F32)
        want = given_ref[s, ROWS:].astype(F32)
        for b in range(BLOCKS):
            totals[b] = totals[b] + jnp.where(want == b + 1.0, got, 0.0)
    for b in range(BLOCKS):
        out_ref[b] = totals[b]


def turn_kernel(tp_ref, part_ref, out_ref):
    flip = tp_ref[0] & 1
    for m in range(PEERS // 2):
        two = part_ref[:, m * LANES : (m + 1) * LANES].astype(F32).T.astype(BF16)
        for n in range(2):
            q = 2 * m + n
            at = jnp.where(flip == 0, q, (q & 7) * SIDE + (q >> 3))
            out_ref[at] = two[n * BLOCK : (n + 1) * BLOCK]


def fold_kernel(parts_ref, out_ref):
    for q in range(SIDE):
        total = parts_ref[0, q].astype(F32)
        for i in range(1, SIDE):
            total = total + parts_ref[i, q].astype(F32)
        out_ref[q] = total.astype(BF16)


def pack_kernel(q_ref, g_ref, o_ref, log_ref, out_ref):
    out_ref[0:TOK] = q_ref[...]
    out_ref[TOK : 2 * TOK] = g_ref[...]
    prod = (g_ref[...].astype(F32) * o_ref[...].astype(F32)).T
    half = LANES // 2
    stats = jnp.concatenate(
        [
            log_ref[...],
            jnp.sum(prod[:half], axis=0, keepdims=True),
            jnp.sum(prod[half:], axis=0, keepdims=True),
        ],
        axis=0,
    )
    rest = jnp.concatenate([stats[:, m * LANES : (m + 1) * LANES] for m in range(4)], axis=0)
    for n in range(3):
        part = rest.astype(BF16)
        out_ref[2 * TOK + 16 * n : 2 * TOK + 16 * (n + 1)] = part
        rest = rest - part.astype(F32)


def attend_kernel(
    slot_ref,
    home_ref,
    rel_ref,
    fetched_ref,
    piece_ref,
    want_ref,
    q0,
    q1,
    q2,
    q3,
    qp_ref,
    away_ref,
    own_ref,
    gq_own_ref,
    gq_far_ref,
    stats_tab,
    table,
    acc,
):
    near = (q0, q1, q2, q3)
    table[:PEERS] = fetched_ref[...].astype(F32)
    table[PEERS:] = piece_ref[...].astype(F32)
    acc[...] = jnp.zeros(acc.shape, F32)
    low = low_lanes((LANES, LANES))
    low4 = low_lanes((4, LANES))
    row8 = lax.broadcasted_iota(jnp.int32, (ROWS, LANES), 0)
    query_t = lax.broadcasted_iota(jnp.int32, (LANES, LANES), 1) & (BLOCK - 1)

    def stat(p):
        parts = []
        for n in range(3):
            at = 2 * TOK + 16 * n
            parts.append((near[p][at : at + 16, :] if p < 4 else qp_ref[p - 4, at : at + 16, :]).astype(F32))
        total = parts[0] + parts[1] + parts[2]
        kind = lax.broadcasted_iota(jnp.int32, total.shape, 0) & 3
        return total * jnp.where(kind < 2, LOG2E, SCALE)

    for pair in range(4):
        even, odd = stat(2 * pair), stat(2 * pair + 1)
        even_turned = pltpu.roll(even, LANES // 2, 1)
        odd_turned = pltpu.roll(odd, LANES // 2, 1)
        for j in range(BLOCKS):
            m = 4 * (j // 2)
            lo = even[m : m + 4] if j % 2 == 0 else even_turned[m : m + 4]
            hi = odd_turned[m : m + 4] if j % 2 == 0 else odd[m : m + 4]
            stats_tab[j, 0:4, pair * LANES : (pair + 1) * LANES] = jnp.where(low4, lo, hi)

    def one_block(j, carry):
        kv = jnp.concatenate([table[slot_ref[j, s]] for s in range(SLOTS)], axis=0)
        turned = pltpu.roll(kv, LANES // 2, 1)
        scaled = turned * SCALE
        kept = kv * SCALE
        k2 = jnp.concatenate([jnp.where(low, kv, 0.0), jnp.where(low, 0.0, turned)], axis=0).astype(BF16)
        v2 = jnp.concatenate([jnp.where(low, scaled, 0.0), jnp.where(low, 0.0, kept)], axis=0).astype(BF16)
        at = pl.multiple_of(j * BLOCK, BLOCK)
        q = jnp.concatenate(
            [r[pl.ds(at, BLOCK), :] for r in near]
            + [qp_ref[k, pl.ds(at, BLOCK), :] for k in range(4)],
            axis=0,
        )
        g = jnp.concatenate(
            [r[pl.ds(TOK + at, BLOCK), :] for r in near]
            + [qp_ref[k, pl.ds(TOK + at, BLOCK), :] for k in range(4)],
            axis=0,
        )
        last = (((1,), (1,)), ((), ()))
        scores = lax.dot_general(k2, q, last, preferred_element_type=F32)
        dprobs = lax.dot_general(v2, g, last, preferred_element_type=F32)
        rel = jnp.concatenate([row8 + rel_ref[j, s] for s in range(SLOTS)], axis=0)
        seen = (rel <= query_t).astype(F32)
        seen = jnp.concatenate([seen] * 4, axis=1) > 0.0
        stat_j = stats_tab[j]
        probs = []
        dscores = []
        for h in range(2):
            s = scores[h * LANES : (h + 1) * LANES]
            d = dprobs[h * LANES : (h + 1) * LANES]
            p = jnp.where(seen, jnp.exp2(s * (SCALE * LOG2E) - stat_j[h : h + 1, :]), 0.0)
            probs.append(p.astype(BF16))
            dscores.append((p * (d - stat_j[2 + h : 3 + h, :])).astype(BF16))
        probs = jnp.concatenate(probs, axis=0)
        dscores = jnp.concatenate(dscores, axis=0)
        plain = (((1,), (0,)), ((), ()))
        dv = lax.dot_general(probs, g, plain, preferred_element_type=F32)
        dk = lax.dot_general(dscores, q, plain, preferred_element_type=F32)
        gq = lax.dot_general(dscores, k2, (((0,), (0,)), ((), ())), preferred_element_type=F32)
        for k in range(4):
            gq_own_ref[k, pl.ds(at, BLOCK), :] = gq[k * BLOCK : (k + 1) * BLOCK]
            gq_far_ref[k, pl.ds(at, BLOCK), :] = gq[(4 + k) * BLOCK : (5 + k) * BLOCK].astype(BF16)
        both = jnp.where(low, dk[:LANES], dv[LANES:]) + pltpu.roll(
            jnp.where(low, dv[:LANES], dk[LANES:]), LANES // 2, 1
        )
        for s in range(SLOTS):
            acc[home_ref[j, s]] += both[s * ROWS : (s + 1) * ROWS]
        return carry

    def some_blocks(i, carry):
        for n in range(2):
            one_block(i * 2 + n, carry)
        return carry

    lax.fori_loop(0, BLOCKS // 2, some_blocks, 0)
    away_ref[:, :ROWS] = acc[:PEERS].astype(BF16)
    for s in range(PEERS):
        want = jnp.broadcast_to(want_ref[s : s + 1, :], (ROWS, LANES))
        away_ref[s, ROWS:] = want.astype(BF16)
    own_ref[...] = acc[PEERS:]


def place_kernel(tp_ref, near_ref, far_ref, keys_ref, vals_ref, rows):
    x = tp_ref[0] >> 1
    mine = jnp.full((ROWS, LANES), tp_ref[0] & 1, jnp.int32)
    for xa in range(4):
        k = (x + 4 - xa) & 3
        for ca in range(2):
            for b in range(BLOCKS):
                at = b * BLOCK + (xa * 2 + ca) * ROWS
                rows[at : at + ROWS, :] = jnp.where(mine == ca, near_ref[k, b], far_ref[k, b])
    turned = rows[...].T
    keys_ref[...] = turned[: LANES // 2]
    vals_ref[...] = turned[LANES // 2 :]


def call(kernel, ins, out_shape, args, flops, limit=8 << 20, **kw):
    many = isinstance(out_shape, (list, tuple))
    return pl.pallas_call(
        kernel,
        in_specs=ins,
        out_specs=[VMEM] * len(out_shape) if many else VMEM,
        out_shape=out_shape,
        cost_estimate=pl.CostEstimate(flops=flops, bytes_accessed=1 << 20, transcendentals=0),
        compiler_params=pltpu.CompilerParams(vmem_limit_bytes=limit),
        **kw,
    )(*args)


def sds(shape, dtype):
    return jax.ShapeDtypeStruct(shape, dtype)


def held(shape, dtype):
    return pltpu.VMEM(shape, dtype)


def x_from(arr, k):
    return lax.ppermute(arr, "x", [(i, (i + k) % 4) for i in range(4)])


def x_back(arr, k):
    return lax.ppermute(arr, "x", [((i + k) % 4, i) for i in range(4)])


def swap(arr):
    return lax.ppermute(arr, "c", [(0, 1), (1, 0)])


def device(z, y, x, c):
    return ((z * 8 + y) * 4 + x) * 2 + c


def lines(first):
    out = []
    for x in range(4):
        for c in range(2):
            for a in range(SIDE):
                if (c == 0) == first:
                    out.append([device(i, a, x, c) for i in range(SIDE)])
                else:
                    out.append([device(a, i, x, c) for i in range(SIDE)])
    return out


def along(arr, first):
    return lax.all_to_all(
        arr, ALL, split_axis=0, concat_axis=0, tiled=True, axis_index_groups=lines(first)
    )


def exchange(arr):
    return lax.all_to_all(arr, KV, split_axis=0, concat_axis=0, tiled=True)


def near_core(arr):
    return pltpu.with_memory_space_constraint(arr, pltpu.VMEM)


def step(normed, queries, keys, values, attended, cotangent, log_sum, chosen):
    rank = lax.axis_index(KV).astype(jnp.int32)
    x = lax.axis_index("x").astype(jnp.int32)
    c = lax.axis_index("c").astype(jnp.int32)
    tp = x * 2 + c
    offer, piece, want = call(
        offer_kernel,
        [SMEM] * 2 + [VMEM] * 3,
        [
            sds((SIDE, BLOCKS + 1, ROWS, LANES), BF16),
            sds((BLOCKS, ROWS, LANES), BF16),
            sds((PEERS, LANES), F32),
        ],
        (rank.reshape(1), tp.reshape(1), keys.T, values.T, chosen),
        1 << 18,
        limit=58 << 20,
        scratch_shapes=[pltpu.VMEM((TOK, LANES), F32)],
        name="offer",
    )
    pushed = along(offer, True)
    wants = swap(pushed[:, BLOCKS])
    picked = call(
        pick_kernel,
        [VMEM] * 2,
        held((SIDE, SIDE, ROWS, LANES), BF16),
        (near_core(wants), near_core(pushed)),
        1 << 20,
        name="pick",
    )
    fetched = along(picked, False).reshape(PEERS, ROWS, LANES)

    qd = call(
        pack_kernel,
        [VMEM] * 4,
        sds((2 * TOK + 48, LANES), BF16),
        (queries, cotangent, attended, log_sum.T),
        1 << 18,
        limit=58 << 20,
        name="pack",
    )
    qds = [qd] + [x_from(qd, k) for k in (1, 2, 3)]
    qd_far = swap(jnp.stack(qds))

    owner = chosen >> 3
    inner = chosen & 7
    listed = chosen >= 0
    peer = jnp.where(c == 0, (owner & 7) * 8 + (owner >> 3), owner)
    slot = jnp.where(listed, jnp.where(owner == rank, PEERS + inner, peer), 0)
    starts = rank * TOK + lax.broadcasted_iota(jnp.int32, chosen.shape, 0) * BLOCK
    home = jnp.where(listed, jnp.where(owner == rank, PEERS + inner, owner), 0)
    rel = jnp.where(listed, chosen * BLOCK + ROWS * tp - starts, FAR)

    away, own, gq_own, gq_far = call(
        attend_kernel,
        [SMEM] * 3 + [VMEM] * 8,
        [
            held((PEERS, 2 * ROWS, LANES), BF16),
            held((BLOCKS, ROWS, LANES), F32),
            held((4, TOK, LANES), F32),
            held((4, TOK, LANES), BF16),
        ],
        (slot, home, rel, near_core(fetched), near_core(piece), near_core(want), *map(near_core, qds), near_core(qd_far)),
        1 << 30,
        limit=16 << 20,
        scratch_shapes=[
            pltpu.VMEM((BLOCKS, 8, TOK), F32),
            pltpu.VMEM((PEERS + BLOCKS, ROWS, LANES), F32),
            pltpu.VMEM((PEERS + BLOCKS, ROWS, LANES), F32),
        ],
        name="attend",
    )
    gq4 = gq_own + swap(gq_far).astype(F32)
    returned = exchange(away)
    gq = gq4[0]
    for k in (1, 2, 3):
        gq = gq + x_back(gq4[k].astype(BF16), k).astype(F32)
    grad_queries = gq.astype(BF16)
    part = lax.dot_general(
        grad_queries, normed, (((0,), (0,)), ((), ())), preferred_element_type=F32
    ).astype(BF16)
    turned = call(
        turn_kernel,
        [SMEM, VMEM],
        held((PEERS, BLOCK, LANES), BF16),
        (tp.reshape(1), near_core(part)),
        1 << 20,
        name="turn",
    )
    parts = along(turned.reshape(SIDE, SIDE, BLOCK, LANES), True)
    half = call(
        fold_kernel,
        [VMEM],
        held((SIDE, BLOCK, LANES), BF16),
        (near_core(parts),),
        1 << 20,
        name="fold",
    )
    parts = along(half, False)
    weight_grad = jnp.sum(parts.astype(F32), axis=0)

    total = call(
        settle_kernel,
        [VMEM] * 2,
        held((BLOCKS, ROWS, LANES), F32),
        (near_core(own), near_core(returned)),
        1 << 20,
        name="settle",
    )
    near = jnp.stack([total] + [x_from(total, k) for k in (1, 2, 3)])
    far = swap(near)
    grad_keys, grad_values = call(
        place_kernel,
        [SMEM, VMEM, VMEM],
        [sds((64, TOK), F32), sds((64, TOK), F32)],
        (tp.reshape(1), near_core(near), near_core(far)),
        1 << 20,
        scratch_shapes=[pltpu.VMEM((TOK, LANES), F32)],
        name="place",
    )
    return grad_queries, grad_keys.T, grad_values.T, weight_grad


def solution(mesh):
    torus = Mesh(mesh.devices.reshape(8, 8, 4, 2), ("z", "y", "x", "c"))
    heads = ("x", "c")
    in_specs = (
        P(KV, None),
        P(KV, heads),
        P(KV, None),
        P(KV, None),
        P(KV, heads),
        P(KV, heads),
        P(KV, heads),
        P(KV, None),
    )
    out_specs = (P(KV, heads), P(KV, None), P(KV, None), P(KV, heads))
    return jax.shard_map(step, mesh=torus, in_specs=in_specs, out_specs=out_specs, check_vma=False)
```

```python
import jax
import jax.numpy as jnp
from jax import lax
from jax.experimental import pallas as pl
from jax.experimental.pallas import tpu as pltpu
from jax.sharding import Mesh
from jax.sharding import PartitionSpec as P


BLOCK = 64
BLOCKS = 8
SLOTS = 16
PEERS = 64
SIDE = 8
ROWS = 8
TOK = 512
LANES = 128
SCALE = 0.125
LOG2E = 1.4426950408889634
KV = ("z", "y")
ALL = ("z", "y", "x", "c")
FAR = 1 << 20
F32 = jnp.float32
BF16 = jnp.bfloat16
VMEM = pl.BlockSpec(memory_space=pltpu.VMEM)
SMEM = pl.BlockSpec(memory_space=pltpu.SMEM)


def low_lanes(shape):
    return lax.broadcasted_iota(jnp.int32, shape, len(shape) - 1) < LANES // 2


def offer_kernel(rank_ref, tp_ref, keys_ref, vals_ref, chosen_ref, out_ref, piece_ref, want_ref, pairs):
    rank = rank_ref[0]
    tp = tp_ref[0]
    flip = tp & 1
    both = jnp.concatenate([keys_ref[...], vals_ref[...]], axis=0).astype(F32)
    pairs[...] = both.T
    at = lax.broadcasted_iota(jnp.int32, (PEERS, SLOTS), 0)

    def wanted(peer):
        best = jnp.zeros((PEERS, SLOTS), jnp.int32)
        for j in range(BLOCKS):
            c = chosen_ref[j : j + 1, :]
            hit = ((c >> 3) == peer) & (c >= 0) & (peer != rank)
            best = jnp.maximum(best, jnp.where(hit, (c & 7) + 1, 0))
        best = jnp.max(best, axis=1, keepdims=True)
        return jnp.broadcast_to(best, (PEERS, LANES)).astype(F32)

    best = wanted(jnp.where(jnp.full(at.shape, flip, jnp.int32) == 0, at, (at & 7) * 8 + (at >> 3)))
    want_ref[...] = wanted(at)
    for b in range(BLOCKS):
        at = pl.multiple_of(b * BLOCK + tp * ROWS, ROWS)
        piece = pairs[pl.ds(at, ROWS), :].astype(BF16)
        piece_ref[b] = piece
        for i in range(SIDE):
            out_ref[i, b] = piece
    for i in range(SIDE):
        out_ref[i, BLOCKS] = best[i * SIDE : (i + 1) * SIDE].astype(BF16)


def pick_kernel(wants_ref, pushed_ref, out_ref):
    for r in range(SIDE):
        pieces = [pushed_ref[r, b].astype(F32) for b in range(BLOCKS)]
        for i in range(SIDE):
            want = jnp.broadcast_to(wants_ref[i].astype(F32)[r : r + 1], (ROWS, LANES))
            got = jnp.zeros((ROWS, LANES), F32)
            for b in range(BLOCKS):
                got = jnp.where(want == b + 1.0, pieces[b], got)
            out_ref[i, r] = got.astype(BF16)


def settle_kernel(own_ref, given_ref, out_ref):
    totals = [own_ref[b] for b in range(BLOCKS)]
    for s in range(PEERS):
        got = given_ref[s, :ROWS].astype(F32)
        want = given_ref[s, ROWS:].astype(F32)
        for b in range(BLOCKS):
            totals[b] = totals[b] + jnp.where(want == b + 1.0, got, 0.0)
    for b in range(BLOCKS):
        out_ref[b] = totals[b]


def pack_kernel(q_ref, g_ref, o_ref, log_ref, out_ref):
    out_ref[0:TOK] = q_ref[...]
    out_ref[TOK : 2 * TOK] = g_ref[...]
    prod = (g_ref[...].astype(F32) * o_ref[...].astype(F32)).T
    half = LANES // 2
    stats = jnp.concatenate(
        [
            log_ref[...],
            jnp.sum(prod[:half], axis=0, keepdims=True),
            jnp.sum(prod[half:], axis=0, keepdims=True),
        ],
        axis=0,
    )
    rest = jnp.concatenate([stats[:, m * LANES : (m + 1) * LANES] for m in range(4)], axis=0)
    for n in range(3):
        part = rest.astype(BF16)
        out_ref[2 * TOK + 16 * n : 2 * TOK + 16 * (n + 1)] = part
        rest = rest - part.astype(F32)


def attend_kernel(
    slot_ref,
    home_ref,
    rel_ref,
    fetched_ref,
    piece_ref,
    want_ref,
    q0,
    q1,
    q2,
    q3,
    qp_ref,
    away_ref,
    own_ref,
    gq_own_ref,
    gq_far_ref,
    stats_tab,
    table,
    acc,
):
    near = (q0, q1, q2, q3)
    table[:PEERS] = fetched_ref[...].astype(F32)
    table[PEERS:] = piece_ref[...].astype(F32)
    acc[...] = jnp.zeros(acc.shape, F32)
    low = low_lanes((LANES, LANES))
    low4 = low_lanes((4, LANES))
    row8 = lax.broadcasted_iota(jnp.int32, (ROWS, LANES), 0)
    query_t = lax.broadcasted_iota(jnp.int32, (LANES, LANES), 1) & (BLOCK - 1)

    def stat(p):
        parts = []
        for n in range(3):
            at = 2 * TOK + 16 * n
            parts.append((near[p][at : at + 16, :] if p < 4 else qp_ref[p - 4, at : at + 16, :]).astype(F32))
        total = parts[0] + parts[1] + parts[2]
        kind = lax.broadcasted_iota(jnp.int32, total.shape, 0) & 3
        return total * jnp.where(kind < 2, LOG2E, SCALE)

    for pair in range(4):
        even, odd = stat(2 * pair), stat(2 * pair + 1)
        even_turned = pltpu.roll(even, LANES // 2, 1)
        odd_turned = pltpu.roll(odd, LANES // 2, 1)
        for j in range(BLOCKS):
            m = 4 * (j // 2)
            lo = even[m : m + 4] if j % 2 == 0 else even_turned[m : m + 4]
            hi = odd_turned[m : m + 4] if j % 2 == 0 else odd[m : m + 4]
            stats_tab[j, 0:4, pair * LANES : (pair + 1) * LANES] = jnp.where(low4, lo, hi)

    def one_block(j, carry):
        kv = jnp.concatenate([table[slot_ref[j, s]] for s in range(SLOTS)], axis=0)
        turned = pltpu.roll(kv, LANES // 2, 1)
        scaled = turned * SCALE
        kept = kv * SCALE
        k2 = jnp.concatenate([jnp.where(low, kv, 0.0), jnp.where(low, 0.0, turned)], axis=0).astype(BF16)
        v2 = jnp.concatenate([jnp.where(low, scaled, 0.0), jnp.where(low, 0.0, kept)], axis=0).astype(BF16)
        at = pl.multiple_of(j * BLOCK, BLOCK)
        q = jnp.concatenate(
            [r[pl.ds(at, BLOCK), :] for r in near]
            + [qp_ref[k, pl.ds(at, BLOCK), :] for k in range(4)],
            axis=0,
        )
        g = jnp.concatenate(
            [r[pl.ds(TOK + at, BLOCK), :] for r in near]
            + [qp_ref[k, pl.ds(TOK + at, BLOCK), :] for k in range(4)],
            axis=0,
        )
        last = (((1,), (1,)), ((), ()))
        scores = lax.dot_general(k2, q, last, preferred_element_type=F32)
        dprobs = lax.dot_general(v2, g, last, preferred_element_type=F32)
        rel = jnp.concatenate([row8 + rel_ref[j, s] for s in range(SLOTS)], axis=0)
        seen = (rel <= query_t).astype(F32)
        seen = jnp.concatenate([seen] * 4, axis=1) > 0.0
        stat_j = stats_tab[j]
        probs = []
        dscores = []
        for h in range(2):
            s = scores[h * LANES : (h + 1) * LANES]
            d = dprobs[h * LANES : (h + 1) * LANES]
            p = jnp.where(seen, jnp.exp2(s * (SCALE * LOG2E) - stat_j[h : h + 1, :]), 0.0)
            probs.append(p.astype(BF16))
            dscores.append((p * (d - stat_j[2 + h : 3 + h, :])).astype(BF16))
        probs = jnp.concatenate(probs, axis=0)
        dscores = jnp.concatenate(dscores, axis=0)
        plain = (((1,), (0,)), ((), ()))
        dv = lax.dot_general(probs, g, plain, preferred_element_type=F32)
        dk = lax.dot_general(dscores, q, plain, preferred_element_type=F32)
        gq = lax.dot_general(dscores, k2, (((0,), (0,)), ((), ())), preferred_element_type=F32)
        for k in range(4):
            gq_own_ref[k, pl.ds(at, BLOCK), :] = gq[k * BLOCK : (k + 1) * BLOCK]
            gq_far_ref[k, pl.ds(at, BLOCK), :] = gq[(4 + k) * BLOCK : (5 + k) * BLOCK].astype(BF16)
        both = jnp.where(low, dk[:LANES], dv[LANES:]) + pltpu.roll(
            jnp.where(low, dv[:LANES], dk[LANES:]), LANES // 2, 1
        )
        for s in range(SLOTS):
            acc[home_ref[j, s]] += both[s * ROWS : (s + 1) * ROWS]
        return carry

    def some_blocks(i, carry):
        for n in range(4):
            one_block(i * 4 + n, carry)
        return carry

    lax.fori_loop(0, BLOCKS // 4, some_blocks, 0)
    away_ref[:, :ROWS] = acc[:PEERS].astype(BF16)
    for s in range(PEERS):
        want = jnp.broadcast_to(want_ref[s : s + 1, :], (ROWS, LANES))
        away_ref[s, ROWS:] = want.astype(BF16)
    own_ref[...] = acc[PEERS:]


def place_kernel(tp_ref, near_ref, far_ref, keys_ref, vals_ref, rows):
    x = tp_ref[0] >> 1
    mine = jnp.full((ROWS, LANES), tp_ref[0] & 1, jnp.int32)
    for xa in range(4):
        k = (x + 4 - xa) & 3
        for ca in range(2):
            for b in range(BLOCKS):
                at = b * BLOCK + (xa * 2 + ca) * ROWS
                rows[at : at + ROWS, :] = jnp.where(mine == ca, near_ref[k, b], far_ref[k, b])
    turned = rows[...].T
    keys_ref[...] = turned[: LANES // 2]
    vals_ref[...] = turned[LANES // 2 :]


def call(kernel, ins, out_shape, args, flops, limit=8 << 20, **kw):
    many = isinstance(out_shape, (list, tuple))
    return pl.pallas_call(
        kernel,
        in_specs=ins,
        out_specs=[VMEM] * len(out_shape) if many else VMEM,
        out_shape=out_shape,
        cost_estimate=pl.CostEstimate(flops=flops, bytes_accessed=1 << 20, transcendentals=0),
        compiler_params=pltpu.CompilerParams(vmem_limit_bytes=limit),
        **kw,
    )(*args)


def sds(shape, dtype):
    return jax.ShapeDtypeStruct(shape, dtype)


def held(shape, dtype):
    return pltpu.VMEM(shape, dtype)


def x_from(arr, k):
    return lax.ppermute(arr, "x", [(i, (i + k) % 4) for i in range(4)])


def x_back(arr, k):
    return lax.ppermute(arr, "x", [((i + k) % 4, i) for i in range(4)])


def swap(arr):
    return lax.ppermute(arr, "c", [(0, 1), (1, 0)])


def device(z, y, x, c):
    return ((z * 8 + y) * 4 + x) * 2 + c


def lines(first):
    out = []
    for x in range(4):
        for c in range(2):
            for a in range(SIDE):
                if (c == 0) == first:
                    out.append([device(i, a, x, c) for i in range(SIDE)])
                else:
                    out.append([device(a, i, x, c) for i in range(SIDE)])
    return out


def along(arr, first):
    return lax.all_to_all(
        arr, ALL, split_axis=0, concat_axis=0, tiled=True, axis_index_groups=lines(first)
    )


def exchange(arr):
    return lax.all_to_all(arr, KV, split_axis=0, concat_axis=0, tiled=True)


def near_core(arr):
    return pltpu.with_memory_space_constraint(arr, pltpu.VMEM)


def step(normed, queries, keys, values, attended, cotangent, log_sum, chosen):
    rank = lax.axis_index(KV).astype(jnp.int32)
    x = lax.axis_index("x").astype(jnp.int32)
    c = lax.axis_index("c").astype(jnp.int32)
    tp = x * 2 + c
    offer, piece, want = call(
        offer_kernel,
        [SMEM] * 2 + [VMEM] * 3,
        [
            sds((SIDE, BLOCKS + 1, ROWS, LANES), BF16),
            sds((BLOCKS, ROWS, LANES), BF16),
            sds((PEERS, LANES), F32),
        ],
        (rank.reshape(1), tp.reshape(1), keys.T, values.T, chosen),
        1 << 18,
        limit=58 << 20,
        scratch_shapes=[pltpu.VMEM((TOK, LANES), F32)],
        name="offer",
    )
    pushed = along(offer, True)
    wants = swap(pushed[:, BLOCKS])
    picked = call(
        pick_kernel,
        [VMEM] * 2,
        held((SIDE, SIDE, ROWS, LANES), BF16),
        (near_core(wants), near_core(pushed)),
        1 << 20,
        name="pick",
    )
    fetched = along(picked, False).reshape(PEERS, ROWS, LANES)

    qd = call(
        pack_kernel,
        [VMEM] * 4,
        sds((2 * TOK + 48, LANES), BF16),
        (queries, cotangent, attended, log_sum.T),
        1 << 18,
        limit=58 << 20,
        name="pack",
    )
    qds = [qd] + [x_from(qd, k) for k in (1, 2, 3)]
    qd_far = swap(jnp.stack(qds))

    owner = chosen >> 3
    inner = chosen & 7
    listed = chosen >= 0
    peer = jnp.where(c == 0, (owner & 7) * 8 + (owner >> 3), owner)
    slot = jnp.where(listed, jnp.where(owner == rank, PEERS + inner, peer), 0)
    starts = rank * TOK + lax.broadcasted_iota(jnp.int32, chosen.shape, 0) * BLOCK
    home = jnp.where(listed, jnp.where(owner == rank, PEERS + inner, owner), 0)
    rel = jnp.where(listed, chosen * BLOCK + ROWS * tp - starts, FAR)

    away, own, gq_own, gq_far = call(
        attend_kernel,
        [SMEM] * 3 + [VMEM] * 8,
        [
            held((PEERS, 2 * ROWS, LANES), BF16),
            held((BLOCKS, ROWS, LANES), F32),
            held((4, TOK, LANES), F32),
            held((4, TOK, LANES), BF16),
        ],
        (slot, home, rel, near_core(fetched), near_core(piece), near_core(want), *map(near_core, qds), near_core(qd_far)),
        1 << 30,
        limit=16 << 20,
        scratch_shapes=[
            pltpu.VMEM((BLOCKS, 8, TOK), F32),
            pltpu.VMEM((PEERS + BLOCKS, ROWS, LANES), F32),
            pltpu.VMEM((PEERS + BLOCKS, ROWS, LANES), F32),
        ],
        name="attend",
    )
    gq4 = gq_own + swap(gq_far).astype(F32)
    returned = exchange(away)
    gq = gq4[0]
    for k in (1, 2, 3):
        gq = gq + x_back(gq4[k].astype(BF16), k).astype(F32)
    grad_queries = gq.astype(BF16)
    part = lax.dot_general(
        normed, grad_queries, (((0,), (0,)), ((), ())), preferred_element_type=F32
    ).astype(BF16)
    parts = exchange(part.reshape(PEERS, BLOCK, LANES))
    weight_grad = jnp.sum(parts.astype(F32), axis=0)

    total = call(
        settle_kernel,
        [VMEM] * 2,
        held((BLOCKS, ROWS, LANES), F32),
        (near_core(own), near_core(returned)),
        1 << 20,
        name="settle",
    )
    near = jnp.stack([total] + [x_from(total, k) for k in (1, 2, 3)])
    far = swap(near)
    grad_keys, grad_values = call(
        place_kernel,
        [SMEM, VMEM, VMEM],
        [sds((64, TOK), F32), sds((64, TOK), F32)],
        (tp.reshape(1), near_core(near), near_core(far)),
        1 << 20,
        scratch_shapes=[pltpu.VMEM((TOK, LANES), F32)],
        name="place",
    )
    return grad_queries, grad_keys.T, grad_values.T, weight_grad


def solution(mesh):
    torus = Mesh(mesh.devices.reshape(8, 8, 4, 2), ("z", "y", "x", "c"))
    heads = ("x", "c")
    in_specs = (
        P(KV, None),
        P(KV, heads),
        P(KV, None),
        P(KV, None),
        P(KV, heads),
        P(KV, heads),
        P(KV, heads),
        P(KV, None),
    )
    out_specs = (P(KV, heads), P(KV, None), P(KV, None), P(KV, heads))
    return jax.shard_map(step, mesh=torus, in_specs=in_specs, out_specs=out_specs, check_vma=False)
```

```python
import jax
import jax.numpy as jnp
from jax import lax
from jax.experimental import pallas as pl
from jax.experimental.pallas import tpu as pltpu
from jax.sharding import Mesh
from jax.sharding import PartitionSpec as P


BLOCK = 64
BLOCKS = 8
SLOTS = 16
PEERS = 64
SIDE = 8
ROWS = 8
TOK = 512
LANES = 128
SCALE = 0.125
LOG2E = 1.4426950408889634
KV = ("z", "y")
TP = ("x", "c")
ALL = ("z", "y", "x", "c")
FAR = 1 << 20
F32 = jnp.float32
BF16 = jnp.bfloat16
VMEM = pl.BlockSpec(memory_space=pltpu.VMEM)
SMEM = pl.BlockSpec(memory_space=pltpu.SMEM)


def low_lanes(shape):
    return lax.broadcasted_iota(jnp.int32, shape, len(shape) - 1) < LANES // 2


def offer_kernel(rank_ref, tp_ref, keys_ref, vals_ref, chosen_ref, out_ref, piece_ref, pairs):
    rank = rank_ref[0]
    tp = tp_ref[0]
    flip = tp & 1
    both = jnp.concatenate([keys_ref[...], vals_ref[...]], axis=0).astype(F32)
    pairs[...] = both.T
    at = lax.broadcasted_iota(jnp.int32, (PEERS, SLOTS), 0)

    def wanted(peer):
        best = jnp.zeros((PEERS, SLOTS), jnp.int32)
        for j in range(BLOCKS):
            c = chosen_ref[j : j + 1, :]
            hit = ((c >> 3) == peer) & (c >= 0) & (peer != rank)
            best = jnp.maximum(best, jnp.where(hit, (c & 7) + 1, 0))
        best = jnp.max(best, axis=1, keepdims=True)
        return jnp.broadcast_to(best, (PEERS, LANES)).astype(F32)

    best = wanted(jnp.where(jnp.full(at.shape, flip, jnp.int32) == 0, at, (at & 7) * 8 + (at >> 3)))
    for b in range(BLOCKS):
        at = pl.multiple_of(b * BLOCK + tp * ROWS, ROWS)
        piece = pairs[pl.ds(at, ROWS), :].astype(BF16)
        piece_ref[b] = piece
        for i in range(SIDE):
            out_ref[i, b] = piece
    for i in range(SIDE):
        out_ref[i, BLOCKS] = best[i * SIDE : (i + 1) * SIDE].astype(BF16)


def pick_kernel(wants_ref, pushed_ref, out_ref):
    for r in range(SIDE):
        pieces = [pushed_ref[r, b].astype(F32) for b in range(BLOCKS)]
        for i in range(SIDE):
            want = jnp.broadcast_to(wants_ref[i].astype(F32)[r : r + 1], (ROWS, LANES))
            got = jnp.zeros((ROWS, LANES), F32)
            for b in range(BLOCKS):
                got = jnp.where(want == b + 1.0, pieces[b], got)
            out_ref[i, r] = got.astype(BF16)


def turn_kernel(tp_ref, part_ref, away_ref, out_ref):
    flip = tp_ref[0] & 1
    for m in range(PEERS // 2):
        two = part_ref[:, m * LANES : (m + 1) * LANES].astype(F32).T.astype(BF16)
        for n in range(2):
            hi, lo = (2 * m + n) // SIDE, (2 * m + n) % SIDE
            out_ref[jnp.where(flip == 0, lo, hi), jnp.where(flip == 0, hi, lo)] = two[
                n * BLOCK : (n + 1) * BLOCK
            ]
    for i in range(SIDE):
        for r in range(SIDE):
            out_ref[i, SIDE, r * ROWS : (r + 1) * ROWS] = away_ref[i * SIDE + r]


def fold_kernel(wants_ref, parts_ref, out_ref):
    for r in range(SIDE):
        total = parts_ref[0, r].astype(F32)
        for i in range(1, SIDE):
            total = total + parts_ref[i, r].astype(F32)
        out_ref[r, 0] = total.astype(BF16)
        sums = [jnp.zeros((ROWS, LANES), F32) for _ in range(BLOCKS)]
        for i in range(SIDE):
            want = jnp.broadcast_to(wants_ref[i].astype(F32)[r : r + 1], (ROWS, LANES))
            got = parts_ref[i, SIDE, r * ROWS : (r + 1) * ROWS].astype(F32)
            for b in range(BLOCKS):
                sums[b] = sums[b] + jnp.where(want == b + 1.0, got, 0.0)
        for b in range(BLOCKS):
            out_ref[r, 1, b * ROWS : (b + 1) * ROWS] = sums[b].astype(BF16)


def settle_kernel(own_ref, back_ref, out_ref, weight_ref):
    weight = back_ref[0, 0].astype(F32)
    for i in range(1, SIDE):
        weight = weight + back_ref[i, 0].astype(F32)
    weight_ref[...] = weight
    for b in range(BLOCKS):
        total = own_ref[b]
        for i in range(SIDE):
            total = total + back_ref[i, 1, b * ROWS : (b + 1) * ROWS].astype(F32)
        for i in range(SIDE):
            out_ref[i, b] = total


def pack_kernel(q_ref, g_ref, o_ref, log_ref, out_ref):
    out_ref[0:TOK] = q_ref[...]
    out_ref[TOK : 2 * TOK] = g_ref[...]
    prod = (g_ref[...].astype(F32) * o_ref[...].astype(F32)).T
    half = LANES // 2
    stats = jnp.concatenate(
        [
            log_ref[...],
            jnp.sum(prod[:half], axis=0, keepdims=True),
            jnp.sum(prod[half:], axis=0, keepdims=True),
        ],
        axis=0,
    )
    rest = jnp.concatenate([stats[:, m * LANES : (m + 1) * LANES] for m in range(4)], axis=0)
    for n in range(3):
        part = rest.astype(BF16)
        out_ref[2 * TOK + 16 * n : 2 * TOK + 16 * (n + 1)] = part
        rest = rest - part.astype(F32)


def attend_kernel(
    slot_ref,
    tp_ref,
    rel_ref,
    fetched_ref,
    piece_ref,
    q0,
    q1,
    q2,
    q3,
    qp_ref,
    away_ref,
    own_ref,
    gq_own_ref,
    gq_far_ref,
    stats_tab,
    table,
    acc,
):
    near = (q0, q1, q2, q3)
    table[:PEERS] = fetched_ref[...].astype(F32)
    table[PEERS:] = piece_ref[...].astype(F32)
    acc[...] = jnp.zeros(acc.shape, F32)
    low = low_lanes((LANES, LANES))
    low4 = low_lanes((4, LANES))
    row8 = lax.broadcasted_iota(jnp.int32, (ROWS, LANES), 0)
    query_t = lax.broadcasted_iota(jnp.int32, (LANES, LANES), 1) & (BLOCK - 1)

    def stat(p):
        parts = []
        for n in range(3):
            at = 2 * TOK + 16 * n
            parts.append((near[p][at : at + 16, :] if p < 4 else qp_ref[p - 4, at : at + 16, :]).astype(F32))
        total = parts[0] + parts[1] + parts[2]
        kind = lax.broadcasted_iota(jnp.int32, total.shape, 0) & 3
        return total * jnp.where(kind < 2, LOG2E, SCALE)

    for pair in range(4):
        even, odd = stat(2 * pair), stat(2 * pair + 1)
        even_turned = pltpu.roll(even, LANES // 2, 1)
        odd_turned = pltpu.roll(odd, LANES // 2, 1)
        for j in range(BLOCKS):
            m = 4 * (j // 2)
            lo = even[m : m + 4] if j % 2 == 0 else even_turned[m : m + 4]
            hi = odd_turned[m : m + 4] if j % 2 == 0 else odd[m : m + 4]
            stats_tab[j, 0:4, pair * LANES : (pair + 1) * LANES] = jnp.where(low4, lo, hi)

    def one_block(j, carry):
        kv = jnp.concatenate([table[slot_ref[j, s]] for s in range(SLOTS)], axis=0)
        turned = pltpu.roll(kv, LANES // 2, 1)
        scaled = turned * SCALE
        kept = kv * SCALE
        k2 = jnp.concatenate([jnp.where(low, kv, 0.0), jnp.where(low, 0.0, turned)], axis=0).astype(BF16)
        v2 = jnp.concatenate([jnp.where(low, scaled, 0.0), jnp.where(low, 0.0, kept)], axis=0).astype(BF16)
        at = pl.multiple_of(j * BLOCK, BLOCK)
        q = jnp.concatenate(
            [r[pl.ds(at, BLOCK), :] for r in near]
            + [qp_ref[k, pl.ds(at, BLOCK), :] for k in range(4)],
            axis=0,
        )
        g = jnp.concatenate(
            [r[pl.ds(TOK + at, BLOCK), :] for r in near]
            + [qp_ref[k, pl.ds(TOK + at, BLOCK), :] for k in range(4)],
            axis=0,
        )
        last = (((1,), (1,)), ((), ()))
        scores = lax.dot_general(k2, q, last, preferred_element_type=F32)
        dprobs = lax.dot_general(v2, g, last, preferred_element_type=F32)
        rel = jnp.concatenate([row8 + rel_ref[j, s] for s in range(SLOTS)], axis=0)
        seen = (rel <= query_t).astype(F32)
        seen = jnp.concatenate([seen] * 4, axis=1) > 0.0
        stat_j = stats_tab[j]
        probs = []
        dscores = []
        for h in range(2):
            s = scores[h * LANES : (h + 1) * LANES]
            d = dprobs[h * LANES : (h + 1) * LANES]
            p = jnp.where(seen, jnp.exp2(s * (SCALE * LOG2E) - stat_j[h : h + 1, :]), 0.0)
            probs.append(p.astype(BF16))
            dscores.append((p * (d - stat_j[2 + h : 3 + h, :])).astype(BF16))
        probs = jnp.concatenate(probs, axis=0)
        dscores = jnp.concatenate(dscores, axis=0)
        plain = (((1,), (0,)), ((), ()))
        dv = lax.dot_general(probs, g, plain, preferred_element_type=F32)
        dk = lax.dot_general(dscores, q, plain, preferred_element_type=F32)
        gq = lax.dot_general(dscores, k2, (((0,), (0,)), ((), ())), preferred_element_type=F32)
        for k in range(4):
            to = ((tp_ref[0] >> 1) + 4 - k) & 3
            gq_own_ref[to, pl.ds(at, BLOCK), :] = gq[k * BLOCK : (k + 1) * BLOCK]
            gq_far_ref[to, pl.ds(at, BLOCK), :] = gq[(4 + k) * BLOCK : (5 + k) * BLOCK].astype(BF16)
        both = jnp.where(low, dk[:LANES], dv[LANES:]) + pltpu.roll(
            jnp.where(low, dv[:LANES], dk[LANES:]), LANES // 2, 1
        )
        for s in range(SLOTS):
            acc[slot_ref[j, s]] += both[s * ROWS : (s + 1) * ROWS]
        return carry

    def some_blocks(i, carry):
        for n in range(4):
            one_block(i * 4 + n, carry)
        return carry

    lax.fori_loop(0, BLOCKS // 4, some_blocks, 0)
    away_ref[...] = acc[:PEERS].astype(BF16)
    own_ref[...] = acc[PEERS:]


def place_kernel(pieces_ref, keys_ref, vals_ref, rows):
    for i in range(SIDE):
        for b in range(BLOCKS):
            at = b * BLOCK + i * ROWS
            rows[at : at + ROWS, :] = pieces_ref[i, b]
    turned = rows[...].T
    keys_ref[...] = turned[: LANES // 2]
    vals_ref[...] = turned[LANES // 2 :]


def call(kernel, ins, out_shape, args, flops, limit=8 << 20, **kw):
    many = isinstance(out_shape, (list, tuple))
    return pl.pallas_call(
        kernel,
        in_specs=ins,
        out_specs=[VMEM] * len(out_shape) if many else VMEM,
        out_shape=out_shape,
        cost_estimate=pl.CostEstimate(flops=flops, bytes_accessed=1 << 20, transcendentals=0),
        compiler_params=pltpu.CompilerParams(vmem_limit_bytes=limit),
        **kw,
    )(*args)


def sds(shape, dtype):
    return jax.ShapeDtypeStruct(shape, dtype)


def held(shape, dtype):
    return pltpu.VMEM(shape, dtype)


def x_from(arr, k):
    return lax.ppermute(arr, "x", [(i, (i + k) % 4) for i in range(4)])


def swap(arr):
    return lax.ppermute(arr, "c", [(0, 1), (1, 0)])


def device(z, y, x, c):
    return ((z * 8 + y) * 4 + x) * 2 + c


def lines(first):
    out = []
    for x in range(4):
        for c in range(2):
            for a in range(SIDE):
                if (c == 0) == first:
                    out.append([device(i, a, x, c) for i in range(SIDE)])
                else:
                    out.append([device(a, i, x, c) for i in range(SIDE)])
    return out


def along(arr, first):
    return lax.all_to_all(
        arr, ALL, split_axis=0, concat_axis=0, tiled=True, axis_index_groups=lines(first)
    )


def near_core(arr):
    return pltpu.with_memory_space_constraint(arr, pltpu.VMEM)


def step(normed, queries, keys, values, attended, cotangent, log_sum, chosen):
    rank = lax.axis_index(KV).astype(jnp.int32)
    x = lax.axis_index("x").astype(jnp.int32)
    c = lax.axis_index("c").astype(jnp.int32)
    tp = x * 2 + c
    offer, piece = call(
        offer_kernel,
        [SMEM] * 2 + [VMEM] * 3,
        [
            sds((SIDE, BLOCKS + 1, ROWS, LANES), BF16),
            sds((BLOCKS, ROWS, LANES), BF16),
        ],
        (rank.reshape(1), tp.reshape(1), keys.T, values.T, chosen),
        1 << 18,
        limit=58 << 20,
        scratch_shapes=[pltpu.VMEM((TOK, LANES), F32)],
        name="offer",
    )
    pushed = along(offer, True)
    wants = swap(pushed[:, BLOCKS])
    picked = call(
        pick_kernel,
        [VMEM] * 2,
        held((SIDE, SIDE, ROWS, LANES), BF16),
        (near_core(wants), near_core(pushed)),
        1 << 20,
        name="pick",
    )
    fetched = along(picked, False).reshape(PEERS, ROWS, LANES)

    qd = call(
        pack_kernel,
        [VMEM] * 4,
        sds((2 * TOK + 48, LANES), BF16),
        (queries, cotangent, attended, log_sum.T),
        1 << 18,
        limit=58 << 20,
        name="pack",
    )
    qds = [qd] + [x_from(qd, k) for k in (1, 2, 3)]
    qd_far = swap(jnp.stack(qds))

    owner = chosen >> 3
    inner = chosen & 7
    listed = chosen >= 0
    peer = jnp.where(c == 0, (owner & 7) * 8 + (owner >> 3), owner)
    slot = jnp.where(listed, jnp.where(owner == rank, PEERS + inner, peer), 0)
    starts = rank * TOK + lax.broadcasted_iota(jnp.int32, chosen.shape, 0) * BLOCK
    rel = jnp.where(listed, chosen * BLOCK + ROWS * tp - starts, FAR)

    away, own, gq_own, gq_far = call(
        attend_kernel,
        [SMEM] * 3 + [VMEM] * 7,
        [
            held((PEERS, ROWS, LANES), BF16),
            held((BLOCKS, ROWS, LANES), F32),
            held((4, TOK, LANES), F32),
            held((4, TOK, LANES), BF16),
        ],
        (slot, tp.reshape(1), rel, near_core(fetched), near_core(piece), *map(near_core, qds), near_core(qd_far)),
        1 << 30,
        limit=16 << 20,
        scratch_shapes=[
            pltpu.VMEM((BLOCKS, 8, TOK), F32),
            pltpu.VMEM((PEERS + BLOCKS, ROWS, LANES), F32),
            pltpu.VMEM((PEERS + BLOCKS, ROWS, LANES), F32),
        ],
        name="attend",
    )
    gq4 = (gq_own + swap(gq_far).astype(F32)).astype(BF16)
    got = lax.all_to_all(gq4, "x", split_axis=0, concat_axis=0, tiled=True).astype(F32)
    grad_queries = (got[0] + got[1] + (got[2] + got[3])).astype(BF16)
    part = lax.dot_general(
        grad_queries, normed, (((0,), (0,)), ((), ())), preferred_element_type=F32
    ).astype(BF16)
    turned = call(
        turn_kernel,
        [SMEM, VMEM, VMEM],
        held((SIDE, SIDE + 1, BLOCK, LANES), BF16),
        (tp.reshape(1), near_core(part), near_core(away)),
        1 << 20,
        name="turn",
    )
    parts = along(turned, False)
    folded = call(
        fold_kernel,
        [VMEM] * 2,
        held((SIDE, 2, BLOCK, LANES), BF16),
        (near_core(wants), near_core(parts)),
        1 << 20,
        name="fold",
    )
    back = along(folded, True)
    total, weight_grad = call(
        settle_kernel,
        [VMEM] * 2,
        [sds((SIDE, BLOCKS, ROWS, LANES), F32), sds((BLOCK, LANES), F32)],
        (near_core(own), near_core(back)),
        1 << 20,
        name="settle",
    )
    pieces = lax.all_to_all(total, TP, split_axis=0, concat_axis=0, tiled=True)
    grad_keys, grad_values = call(
        place_kernel,
        [VMEM],
        [sds((64, TOK), F32), sds((64, TOK), F32)],
        (near_core(pieces),),
        1 << 20,
        scratch_shapes=[pltpu.VMEM((TOK, LANES), F32)],
        name="place",
    )
    return grad_queries, grad_keys.T, grad_values.T, weight_grad


def solution(mesh):
    torus = Mesh(mesh.devices.reshape(8, 8, 4, 2), ("z", "y", "x", "c"))
    heads = ("x", "c")
    in_specs = (
        P(KV, None),
        P(KV, heads),
        P(KV, None),
        P(KV, None),
        P(KV, heads),
        P(KV, heads),
        P(KV, heads),
        P(KV, None),
    )
    out_specs = (P(KV, heads), P(KV, None), P(KV, None), P(KV, heads))
    return jax.shard_map(step, mesh=torus, in_specs=in_specs, out_specs=out_specs, check_vma=False)
```

```python
import jax
import jax.numpy as jnp
from jax import lax
from jax.experimental import pallas as pl
from jax.experimental.pallas import tpu as pltpu
from jax.sharding import Mesh
from jax.sharding import PartitionSpec as P


BLOCK = 64
BLOCKS = 8
SLOTS = 16
PEERS = 64
SIDE = 8
ROWS = 8
TOK = 512
LANES = 128
SCALE = 0.125
LOG2E = 1.4426950408889634
KV = ("z", "y")
TP = ("x", "c")
ALL = ("z", "y", "x", "c")
FAR = 1 << 20
F32 = jnp.float32
BF16 = jnp.bfloat16
VMEM = pl.BlockSpec(memory_space=pltpu.VMEM)
SMEM = pl.BlockSpec(memory_space=pltpu.SMEM)
ANY = pl.BlockSpec(memory_space=pltpu.HBM)


def low_lanes(shape):
    return lax.broadcasted_iota(jnp.int32, shape, len(shape) - 1) < LANES // 2


def offer_kernel(rank_ref, tp_ref, keys_ref, vals_ref, chosen_ref, out_ref, piece_ref, pairs):
    rank = rank_ref[0]
    tp = tp_ref[0]
    flip = tp & 1
    both = jnp.concatenate([keys_ref[...], vals_ref[...]], axis=0).astype(F32)
    pairs[...] = both.T
    at = lax.broadcasted_iota(jnp.int32, (PEERS, SLOTS), 0)

    def wanted(peer):
        best = jnp.zeros((PEERS, SLOTS), jnp.int32)
        for j in range(BLOCKS):
            c = chosen_ref[j : j + 1, :]
            hit = ((c >> 3) == peer) & (c >= 0) & (peer != rank)
            best = jnp.maximum(best, jnp.where(hit, (c & 7) + 1, 0))
        best = jnp.max(best, axis=1, keepdims=True)
        return jnp.broadcast_to(best, (PEERS, LANES)).astype(F32)

    best = wanted(jnp.where(jnp.full(at.shape, flip, jnp.int32) == 0, at, (at & 7) * 8 + (at >> 3)))
    for b in range(BLOCKS):
        at = pl.multiple_of(b * BLOCK + tp * ROWS, ROWS)
        piece = pairs[pl.ds(at, ROWS), :].astype(BF16)
        piece_ref[b] = piece
        for i in range(SIDE):
            out_ref[i, b] = piece
    for i in range(SIDE):
        out_ref[i, BLOCKS] = best[i * SIDE : (i + 1) * SIDE].astype(BF16)


def pick_kernel(wants_ref, pushed_ref, out_ref):
    for r in range(SIDE):
        pieces = [pushed_ref[r, b].astype(F32) for b in range(BLOCKS)]
        for i in range(SIDE):
            want = jnp.broadcast_to(wants_ref[i].astype(F32)[r : r + 1], (ROWS, LANES))
            got = jnp.zeros((ROWS, LANES), F32)
            for b in range(BLOCKS):
                got = jnp.where(want == b + 1.0, pieces[b], got)
            out_ref[i, r] = got.astype(BF16)


def turn_kernel(tp_ref, part_ref, away_ref, out_ref):
    flip = tp_ref[0] & 1
    for m in range(PEERS // 2):
        two = part_ref[:, m * LANES : (m + 1) * LANES].astype(F32).T.astype(BF16)
        for n in range(2):
            hi, lo = (2 * m + n) // SIDE, (2 * m + n) % SIDE
            out_ref[jnp.where(flip == 0, lo, hi), jnp.where(flip == 0, hi, lo)] = two[
                n * BLOCK : (n + 1) * BLOCK
            ]
    for i in range(SIDE):
        for r in range(SIDE):
            out_ref[i, SIDE, r * ROWS : (r + 1) * ROWS] = away_ref[i * SIDE + r]


def fold_kernel(wants_ref, parts_ref, out_ref):
    for r in range(SIDE):
        total = parts_ref[0, r].astype(F32)
        for i in range(1, SIDE):
            total = total + parts_ref[i, r].astype(F32)
        out_ref[r, 0] = total.astype(BF16)
        sums = [jnp.zeros((ROWS, LANES), F32) for _ in range(BLOCKS)]
        for i in range(SIDE):
            want = jnp.broadcast_to(wants_ref[i].astype(F32)[r : r + 1], (ROWS, LANES))
            got = parts_ref[i, SIDE, r * ROWS : (r + 1) * ROWS].astype(F32)
            for b in range(BLOCKS):
                sums[b] = sums[b] + jnp.where(want == b + 1.0, got, 0.0)
        for b in range(BLOCKS):
            out_ref[r, 1, b * ROWS : (b + 1) * ROWS] = sums[b].astype(BF16)


def settle_kernel(own_ref, back_ref, out_ref, weight_ref):
    weight = back_ref[0, 0].astype(F32)
    for i in range(1, SIDE):
        weight = weight + back_ref[i, 0].astype(F32)
    weight_ref[...] = weight
    for b in range(BLOCKS):
        total = own_ref[b]
        for i in range(SIDE):
            total = total + back_ref[i, 1, b * ROWS : (b + 1) * ROWS].astype(F32)
        for i in range(SIDE):
            out_ref[i, b] = total.astype(BF16)


def pack_kernel(q_ref, g_ref, o_ref, log_ref, out_ref, o_here, log_here, sems):
    moves = [
        pltpu.make_async_copy(q_ref, out_ref.at[pl.ds(0, TOK)], sems.at[0]),
        pltpu.make_async_copy(g_ref, out_ref.at[pl.ds(TOK, TOK)], sems.at[1]),
        pltpu.make_async_copy(o_ref, o_here, sems.at[2]),
        pltpu.make_async_copy(log_ref, log_here, sems.at[3]),
    ]
    for move in moves:
        move.start()
    for move in moves:
        move.wait()
    prod = (out_ref[TOK : 2 * TOK].astype(F32) * o_here[...].astype(F32)).T
    half = LANES // 2
    stats = jnp.concatenate(
        [
            log_here[...],
            jnp.sum(prod[:half], axis=0, keepdims=True),
            jnp.sum(prod[half:], axis=0, keepdims=True),
        ],
        axis=0,
    )
    rest = jnp.concatenate([stats[:, m * LANES : (m + 1) * LANES] for m in range(4)], axis=0)
    for n in range(3):
        part = rest.astype(BF16)
        out_ref[2 * TOK + 16 * n : 2 * TOK + 16 * (n + 1)] = part
        rest = rest - part.astype(F32)


def attend_kernel(
    slot_ref,
    tp_ref,
    rel_ref,
    fetched_ref,
    piece_ref,
    q0,
    q1,
    q2,
    q3,
    qp_ref,
    away_ref,
    own_ref,
    gq_own_ref,
    gq_far_ref,
    stats_tab,
    table,
    acc,
):
    near = (q0, q1, q2, q3)
    table[:PEERS] = fetched_ref[...].astype(F32)
    table[PEERS:] = piece_ref[...].astype(F32)
    acc[...] = jnp.zeros(acc.shape, F32)
    low = low_lanes((LANES, LANES))
    low4 = low_lanes((4, LANES))
    row8 = lax.broadcasted_iota(jnp.int32, (ROWS, LANES), 0)
    query_t = lax.broadcasted_iota(jnp.int32, (LANES, LANES), 1) & (BLOCK - 1)

    def stat(p):
        parts = []
        for n in range(3):
            at = 2 * TOK + 16 * n
            parts.append((near[p][at : at + 16, :] if p < 4 else qp_ref[p - 4, at : at + 16, :]).astype(F32))
        total = parts[0] + parts[1] + parts[2]
        kind = lax.broadcasted_iota(jnp.int32, total.shape, 0) & 3
        return total * jnp.where(kind < 2, LOG2E, SCALE)

    for pair in range(4):
        even, odd = stat(2 * pair), stat(2 * pair + 1)
        even_turned = pltpu.roll(even, LANES // 2, 1)
        odd_turned = pltpu.roll(odd, LANES // 2, 1)
        for j in range(BLOCKS):
            m = 4 * (j // 2)
            lo = even[m : m + 4] if j % 2 == 0 else even_turned[m : m + 4]
            hi = odd_turned[m : m + 4] if j % 2 == 0 else odd[m : m + 4]
            stats_tab[j, 0:4, pair * LANES : (pair + 1) * LANES] = jnp.where(low4, lo, hi)

    def one_block(j, carry):
        kv = jnp.concatenate([table[slot_ref[j, s]] for s in range(SLOTS)], axis=0)
        turned = pltpu.roll(kv, LANES // 2, 1)
        scaled = turned * SCALE
        kept = kv * SCALE
        k2 = jnp.concatenate([jnp.where(low, kv, 0.0), jnp.where(low, 0.0, turned)], axis=0).astype(BF16)
        v2 = jnp.concatenate([jnp.where(low, scaled, 0.0), jnp.where(low, 0.0, kept)], axis=0).astype(BF16)
        at = pl.multiple_of(j * BLOCK, BLOCK)
        q = jnp.concatenate(
            [r[pl.ds(at, BLOCK), :] for r in near]
            + [qp_ref[k, pl.ds(at, BLOCK), :] for k in range(4)],
            axis=0,
        )
        g = jnp.concatenate(
            [r[pl.ds(TOK + at, BLOCK), :] for r in near]
            + [qp_ref[k, pl.ds(TOK + at, BLOCK), :] for k in range(4)],
            axis=0,
        )
        last = (((1,), (1,)), ((), ()))
        scores = lax.dot_general(k2, q, last, preferred_element_type=F32)
        dprobs = lax.dot_general(v2, g, last, preferred_element_type=F32)
        rel = jnp.concatenate([row8 + rel_ref[j, s] for s in range(SLOTS)], axis=0)
        seen = (rel <= query_t).astype(F32)
        seen = jnp.concatenate([seen] * 4, axis=1) > 0.0
        stat_j = stats_tab[j]
        probs = []
        dscores = []
        for h in range(2):
            s = scores[h * LANES : (h + 1) * LANES]
            d = dprobs[h * LANES : (h + 1) * LANES]
            p = jnp.where(seen, jnp.exp2(s * (SCALE * LOG2E) - stat_j[h : h + 1, :]), 0.0)
            probs.append(p.astype(BF16))
            dscores.append((p * (d - stat_j[2 + h : 3 + h, :])).astype(BF16))
        probs = jnp.concatenate(probs, axis=0)
        dscores = jnp.concatenate(dscores, axis=0)
        plain = (((1,), (0,)), ((), ()))
        dv = lax.dot_general(probs, g, plain, preferred_element_type=F32)
        dk = lax.dot_general(dscores, q, plain, preferred_element_type=F32)
        gq = lax.dot_general(dscores, k2, (((0,), (0,)), ((), ())), preferred_element_type=F32)
        for k in range(4):
            to = ((tp_ref[0] >> 1) + 4 - k) & 3
            gq_own_ref[to, pl.ds(at, BLOCK), :] = gq[k * BLOCK : (k + 1) * BLOCK]
            gq_far_ref[to, pl.ds(at, BLOCK), :] = gq[(4 + k) * BLOCK : (5 + k) * BLOCK].astype(BF16)
        both = jnp.where(low, dk[:LANES], dv[LANES:]) + pltpu.roll(
            jnp.where(low, dv[:LANES], dk[LANES:]), LANES // 2, 1
        )
        for s in range(SLOTS):
            acc[slot_ref[j, s]] += both[s * ROWS : (s + 1) * ROWS]
        return carry

    def some_blocks(i, carry):
        for n in range(4):
            one_block(i * 4 + n, carry)
        return carry

    lax.fori_loop(0, BLOCKS // 4, some_blocks, 0)
    away_ref[...] = acc[:PEERS].astype(BF16)
    own_ref[...] = acc[PEERS:]


def place_kernel(pieces_ref, keys_ref, vals_ref, rows):
    for i in range(SIDE):
        for b in range(BLOCKS):
            at = b * BLOCK + i * ROWS
            rows[at : at + ROWS, :] = pieces_ref[i, b].astype(F32)
    turned = rows[...].T
    keys_ref[...] = turned[: LANES // 2]
    vals_ref[...] = turned[LANES // 2 :]


def call(kernel, ins, out_shape, args, flops, limit=8 << 20, **kw):
    many = isinstance(out_shape, (list, tuple))
    return pl.pallas_call(
        kernel,
        in_specs=ins,
        out_specs=[VMEM] * len(out_shape) if many else VMEM,
        out_shape=out_shape,
        cost_estimate=pl.CostEstimate(flops=flops, bytes_accessed=1 << 20, transcendentals=0),
        compiler_params=pltpu.CompilerParams(vmem_limit_bytes=limit),
        **kw,
    )(*args)


def sds(shape, dtype):
    return jax.ShapeDtypeStruct(shape, dtype)


def held(shape, dtype):
    return pltpu.VMEM(shape, dtype)


def x_from(arr, k):
    return lax.ppermute(arr, "x", [(i, (i + k) % 4) for i in range(4)])


def swap(arr):
    return lax.ppermute(arr, "c", [(0, 1), (1, 0)])


def device(z, y, x, c):
    return ((z * 8 + y) * 4 + x) * 2 + c


def lines(first):
    out = []
    for x in range(4):
        for c in range(2):
            for a in range(SIDE):
                if (c == 0) == first:
                    out.append([device(i, a, x, c) for i in range(SIDE)])
                else:
                    out.append([device(a, i, x, c) for i in range(SIDE)])
    return out


def along(arr, first):
    return lax.all_to_all(
        arr, ALL, split_axis=0, concat_axis=0, tiled=True, axis_index_groups=lines(first)
    )


def near_core(arr):
    return pltpu.with_memory_space_constraint(arr, pltpu.VMEM)


def stay(arr):
    return pltpu.with_memory_space_constraint(arr, pltpu.HBM)


def step(normed, queries, keys, values, attended, cotangent, log_sum, chosen):
    rank = lax.axis_index(KV).astype(jnp.int32)
    x = lax.axis_index("x").astype(jnp.int32)
    c = lax.axis_index("c").astype(jnp.int32)
    tp = x * 2 + c
    offer, piece = call(
        offer_kernel,
        [SMEM] * 2 + [VMEM] * 3,
        [
            sds((SIDE, BLOCKS + 1, ROWS, LANES), BF16),
            sds((BLOCKS, ROWS, LANES), BF16),
        ],
        (rank.reshape(1), tp.reshape(1), keys.T, values.T, chosen),
        1 << 18,
        limit=58 << 20,
        scratch_shapes=[pltpu.VMEM((TOK, LANES), F32)],
        name="offer",
    )
    pushed = along(offer, True)
    wants = swap(pushed[:, BLOCKS])
    picked = call(
        pick_kernel,
        [VMEM] * 2,
        held((SIDE, SIDE, ROWS, LANES), BF16),
        (near_core(wants), near_core(pushed)),
        1 << 20,
        name="pick",
    )
    fetched = along(picked, False).reshape(PEERS, ROWS, LANES)

    qd = call(
        pack_kernel,
        [ANY] * 4,
        held((2 * TOK + 48, LANES), BF16),
        tuple(map(stay, (queries, cotangent, attended, log_sum.T))),
        1 << 18,
        scratch_shapes=[
            pltpu.VMEM((TOK, LANES), BF16),
            pltpu.VMEM((2, TOK), F32),
            pltpu.SemaphoreType.DMA((4,)),
        ],
        name="pack",
    )
    first = x_from(qd, 1)
    qds = [qd, first] + [x_from(qd, k) for k in (2, 3)]
    qd_far = swap(jnp.stack(qds))

    owner = chosen >> 3
    inner = chosen & 7
    listed = chosen >= 0
    peer = jnp.where(c == 0, (owner & 7) * 8 + (owner >> 3), owner)
    slot = jnp.where(listed, jnp.where(owner == rank, PEERS + inner, peer), 0)
    starts = rank * TOK + lax.broadcasted_iota(jnp.int32, chosen.shape, 0) * BLOCK
    rel = jnp.where(listed, chosen * BLOCK + ROWS * tp - starts, FAR)

    away, own, gq_own, gq_far = call(
        attend_kernel,
        [SMEM] * 3 + [VMEM] * 7,
        [
            held((PEERS, ROWS, LANES), BF16),
            held((BLOCKS, ROWS, LANES), F32),
            held((4, TOK, LANES), F32),
            held((4, TOK, LANES), BF16),
        ],
        (slot, tp.reshape(1), rel, near_core(fetched), near_core(piece), *map(near_core, qds), near_core(qd_far)),
        1 << 30,
        limit=16 << 20,
        scratch_shapes=[
            pltpu.VMEM((BLOCKS, 8, TOK), F32),
            pltpu.VMEM((PEERS + BLOCKS, ROWS, LANES), F32),
            pltpu.VMEM((PEERS + BLOCKS, ROWS, LANES), F32),
        ],
        name="attend",
    )
    gq4 = (gq_own + swap(gq_far).astype(F32)).astype(BF16)
    got = lax.all_to_all(gq4, "x", split_axis=0, concat_axis=0, tiled=True).astype(F32)
    grad_queries = (got[0] + got[1] + (got[2] + got[3])).astype(BF16)
    part = lax.dot_general(
        grad_queries, normed, (((0,), (0,)), ((), ())), preferred_element_type=F32
    ).astype(BF16)
    turned = call(
        turn_kernel,
        [SMEM, VMEM, VMEM],
        held((SIDE, SIDE + 1, BLOCK, LANES), BF16),
        (tp.reshape(1), near_core(part), near_core(away)),
        1 << 20,
        name="turn",
    )
    parts = along(turned, False)
    folded = call(
        fold_kernel,
        [VMEM] * 2,
        held((SIDE, 2, BLOCK, LANES), BF16),
        (near_core(wants), near_core(parts)),
        1 << 20,
        name="fold",
    )
    back = along(folded, True)
    total, weight_grad = call(
        settle_kernel,
        [VMEM] * 2,
        [held((SIDE, BLOCKS, ROWS, LANES), BF16), sds((BLOCK, LANES), F32)],
        (near_core(own), near_core(back)),
        1 << 20,
        name="settle",
    )
    pieces = lax.all_to_all(total, TP, split_axis=0, concat_axis=0, tiled=True)
    grad_keys, grad_values = call(
        place_kernel,
        [VMEM],
        [sds((64, TOK), F32), sds((64, TOK), F32)],
        (near_core(pieces),),
        1 << 20,
        scratch_shapes=[pltpu.VMEM((TOK, LANES), F32)],
        name="place",
    )
    return grad_queries, grad_keys.T, grad_values.T, weight_grad


def solution(mesh):
    torus = Mesh(mesh.devices.reshape(8, 8, 4, 2), ("z", "y", "x", "c"))
    heads = ("x", "c")
    in_specs = (
        P(KV, None),
        P(KV, heads),
        P(KV, None),
        P(KV, None),
        P(KV, heads),
        P(KV, heads),
        P(KV, heads),
        P(KV, None),
    )
    out_specs = (P(KV, heads), P(KV, None), P(KV, None), P(KV, heads))
    return jax.shard_map(step, mesh=torus, in_specs=in_specs, out_specs=out_specs, check_vma=False)
```
